128 devices in a mesh: kv: 16 (over z, y), tp: 8 (over x, core).
Axes of the slice: x: 4, y: 4, z: 4, core: 2. Of those that a mesh axis runs over, the one named last changes fastest.
Arguments:
- hidden_in: bfloat16 [16, 4096], P(None, ('kv', 'tp')), may hold values from -12 to 12
- attn_gain: float32 [4096], P('kv'), may hold values from 0.1 to 1.9
- query_weight: bfloat16 [4096, 4096], P('kv', 'tp'), may hold values from -0.09375 to 0.09375
- key_cache: bfloat16 [16, 16384, 8, 128], P(None, 'kv', 'tp'), may hold values from -600 to 600
- value_cache: bfloat16 [16, 16384, 8, 128], P(None, 'kv', 'tp'), may hold values from -6 to 6
- lambdas: float32 [32], P('tp'), may hold values from 0.3 to 0.8
- head_gain: float32 [128], replicated, may hold values from 0.1 to 1.9
- out_weight: bfloat16 [4096, 4096], P('tp', 'kv'), may hold values from -0.09375 to 0.09375
- mixer_gain: float32 [4096], P(('kv', 'tp')), may hold values from 0.1 to 1.9
- gate_weight: bfloat16 [4096, 11264], P('kv', 'tp'), may hold values from -0.09375 to 0.09375
- up_weight: bfloat16 [4096, 11264], P('kv', 'tp'), may hold values from -0.09375 to 0.09375
- down_weight: bfloat16 [11264, 4096], P('tp', 'kv'), may hold values from -0.0546875 to 0.0546875
Outputs:
- mixed: bfloat16 [16, 4096], P(None, ('kv', 'tp'))
The draws below stay inside these ranges and needn't reach their ends.
All inputs are finite; a program needn't handle non-finite values.
Results may differ from the reference program's by a relative error of at most 0.017.
Values may be sent and summed in bfloat16 or wider, within the bound.
No kernel may reach another device: no remote copies, remote signals or barrier semaphores. Data moves between devices by JAX's collectives and lax.ppermute only.
A program may use at most 64 MiB of HBM per device.

```python
import jax
import jax.numpy as jnp
from jax import lax

D = 4096
FF = 11264
HEAD_DIM = 64
KV_HEADS = 8
GROUP = 4
HEADS = 32
BATCH = 16
LENGTH = 16384
COLS_DEV = 32
N_TP = 8


def draw_hidden_in(key, part):
    first = jax.random.fold_in(key, 11)
    second = jax.random.fold_in(key, 12)
    blocks = D // COLS_DEV
    ramp = jnp.arange(blocks, dtype=jnp.float32) / max(blocks - 1, 1)
    jitter = jax.random.uniform(second, (blocks,), jnp.float32, -0.15, 0.15)
    block_scale = jnp.exp(jnp.log(0.5) + ramp * jnp.log(6.0) + jitter)
    base = jax.random.normal(first, (BATCH, D), jnp.float32)
    column_scale = jnp.repeat(block_scale, COLS_DEV)
    values = jnp.clip(base * column_scale[None, :], -12.0, 12.0)
    return values.astype(jnp.bfloat16)


def draw_key_cache(key, part):
    first = jax.random.fold_in(key, 21)
    base = 2.0 * jnp.clip(jax.random.normal(first, (BATCH, LENGTH, KV_HEADS, 2 * HEAD_DIM), jnp.float32), -6.0, 6.0)
    return jnp.clip(base, -600.0, 600.0).astype(jnp.bfloat16)


def level_of(stream_key, shape, pieces, least, top_value):
    level, own = 1.0, jax.random.fold_in(stream_key, 6)
    for axis_at, shards_of in pieces:
        steps = jnp.exp(jax.random.uniform(jax.random.fold_in(own, axis_at), (shards_of,), jnp.float32, least / len(pieces), top_value / len(pieces)))
        level = level * jnp.repeat(steps, shape[axis_at] // shards_of).reshape([-1 if axis == axis_at else 1 for axis in range(len(shape))])
    return level


def centred(rng, shape, scale, reach, pieces=(), held_as=jnp.bfloat16):
    result = scale * jax.random.normal(rng, shape, jnp.float32)
    if pieces:
        result = result * level_of(rng, shape, pieces, -0.22, 0.18)
    return jnp.clip(result, -reach, reach).astype(held_as)


def setup_inputs(seed: int = 0) -> dict:
    arg_keys = jax.random.split(jax.random.key(seed), 13)
    hidden_in = draw_hidden_in(jax.random.fold_in(arg_keys[12], 71), 0)
    attn_gain = jnp.clip(1.0 + 0.18 * jax.random.normal(arg_keys[1], (D,), jnp.float32), 0.1, 1.9)
    query_weight = centred(arg_keys[2], (D, HEADS * 2 * HEAD_DIM), D ** -0.5, 0.09375, ((0, 16), (1, 8)))
    key_cache = draw_key_cache(jax.random.fold_in(arg_keys[12], 71), 0)
    value_cache = centred(arg_keys[4], (BATCH, LENGTH, KV_HEADS, 2 * HEAD_DIM), 1.0, 6.0, ((1, 16), (2, 8)))
    lambdas = jnp.clip(0.3 + 0.5 * jax.random.uniform(arg_keys[5], (HEADS,), jnp.float32) ** level_of(arg_keys[5], (HEADS,), ((0, 8),), -0.2, 0.2), 0.3, 0.8)
    head_gain = jnp.clip(1.0 + 0.18 * jax.random.normal(arg_keys[6], (2 * HEAD_DIM,), jnp.float32), 0.1, 1.9)
    out_weight = centred(arg_keys[7], (HEADS * 2 * HEAD_DIM, D), (HEADS * 2 * HEAD_DIM) ** -0.5, 0.09375, ((0, 8), (1, 16)))
    mixer_gain = jnp.clip(1.0 + 0.18 * jax.random.normal(arg_keys[8], (D,), jnp.float32), 0.1, 1.9)
    gate_weight = centred(arg_keys[9], (D, FF), D ** -0.5, 0.09375, ((0, 16), (1, 8)))
    up_weight = centred(arg_keys[10], (D, FF), D ** -0.5, 0.09375, ((0, 16), (1, 8)))
    down_weight = centred(arg_keys[11], (FF, D), FF ** -0.5, 0.0546875, ((0, 8), (1, 16)))
    return {"hidden_in": hidden_in, "attn_gain": attn_gain, "query_weight": query_weight, "key_cache": key_cache, "value_cache": value_cache, "lambdas": lambdas, "head_gain": head_gain, "out_weight": out_weight, "mixer_gain": mixer_gain, "gate_weight": gate_weight, "up_weight": up_weight, "down_weight": down_weight}


eps = 1e-06

def split_sum(activations, weights):
    block_rows = activations.shape[1] // N_TP
    partials = jnp.einsum('bjr,jrd->jbd', activations.reshape(activations.shape[0], N_TP, block_rows).astype(jnp.float32), weights.reshape(N_TP, block_rows, weights.shape[1]).astype(jnp.float32))
    rounded = lax.optimization_barrier(partials.astype(jnp.bfloat16)).astype(jnp.float32)
    return lax.optimization_barrier(jnp.sum(rounded, axis=0))

def reference(hidden_in, attn_gain, query_weight, key_cache, value_cache, lambdas, head_gain, out_weight, mixer_gain, gate_weight, up_weight, down_weight):
    rows_f = hidden_in.astype(jnp.float32)
    inverse = lax.rsqrt(lax.optimization_barrier(jnp.mean(rows_f * rows_f, axis=1, keepdims=True)) + eps)
    gained = (rows_f * attn_gain).astype(jnp.bfloat16)
    query_full = (jnp.dot(gained, query_weight, preferred_element_type=jnp.float32) * inverse).astype(jnp.bfloat16)
    query_heads = query_full.reshape(BATCH, KV_HEADS, GROUP, 2, HEAD_DIM)
    mixing = lambdas.reshape(KV_HEADS, GROUP)

    def one_group(group_index):
        query_part = lax.dynamic_index_in_dim(query_heads, group_index, 1, keepdims=False).astype(jnp.float32)
        key_part = lax.dynamic_index_in_dim(key_cache, group_index, 2, keepdims=False).astype(jnp.float32)
        key_part = key_part.reshape(BATCH, LENGTH, 2, HEAD_DIM)
        value_part = lax.dynamic_index_in_dim(value_cache, group_index, 2, keepdims=False).astype(jnp.float32)
        scores = jnp.einsum('bgcd,blcd->cbgl', query_part, key_part) * HEAD_DIM ** (-0.5)
        maxima = lax.optimization_barrier(jnp.max(scores, axis=-1, keepdims=True))
        exponent = jnp.exp(scores - maxima)
        totals = lax.optimization_barrier(jnp.sum(exponent, axis=-1))
        rounded = lax.optimization_barrier(exponent.astype(jnp.bfloat16)).astype(jnp.float32)
        weighted = jnp.einsum('cbgl,bld->cbgd', rounded, value_part)
        head_means = weighted / totals[..., None]
        lam_row = lax.dynamic_index_in_dim(mixing, group_index, 0, keepdims=False)
        attended = head_means[0] - lam_row[None, :, None] * head_means[1]
        norm_inv = lax.rsqrt(lax.optimization_barrier(jnp.mean(attended * attended, axis=-1, keepdims=True)) + eps)
        return (attended * norm_inv * head_gain).astype(jnp.bfloat16)
    per_group = lax.map(one_group, jnp.arange(KV_HEADS, dtype=jnp.int32))
    head_out = jnp.moveaxis(per_group, 0, 1).reshape(BATCH, HEADS * 2 * HEAD_DIM)
    attn_out = split_sum(head_out, out_weight)
    after_attn = (rows_f + attn_out).astype(jnp.bfloat16)
    after_f = after_attn.astype(jnp.float32)
    inverse_two = lax.rsqrt(lax.optimization_barrier(jnp.mean(after_f * after_f, axis=1, keepdims=True)) + eps)
    mixer_in = (after_f * inverse_two * mixer_gain).astype(jnp.bfloat16)
    gate_sum = jnp.dot(mixer_in, gate_weight, preferred_element_type=jnp.float32)
    up_sum = jnp.dot(mixer_in, up_weight, preferred_element_type=jnp.float32)
    hidden = (jax.nn.silu(gate_sum) * up_sum).astype(jnp.bfloat16)
    mixer_out = split_sum(hidden, down_weight)
    return (after_f + mixer_out).astype(jnp.bfloat16)
```

```python
import jax
import jax.numpy as jnp
from jax import lax
from jax.sharding import Mesh
from jax.sharding import PartitionSpec as P

D = 4096
HEAD_DIM = 64
TP = ("tp_0", "tp_1")
KV = ("kv_0", "kv_1")
KV_TP = ("kv_0", "kv_1", "tp_0", "tp_1")
LANES = 128

eps = 1e-06


def to_all(shard, axis):
    length = lax.axis_size(axis)
    return lax.all_to_all(
        jnp.broadcast_to(shard[None], (length, *shard.shape)), axis, 0, 0, tiled=True
    )


def peers(shard, axis):
    n = lax.axis_size(axis)
    return [
        lax.ppermute(shard, axis, [(i, (i + s) % n) for i in range(n)]) for s in range(1, n)
    ]


def merged(parts):
    tops = [p[0] for p in parts]
    top = tops[0]
    for t in tops[1:]:
        top = jnp.maximum(top, t)
    total, acc = 0.0, 0.0
    for m, t, a in parts:
        f = jnp.exp(m - top)
        total = total + t * f
        acc = acc + a * f[..., None]
    return top, total, acc


def per_device(
    hidden_in,
    attn_gain,
    query_weight,
    key_cache,
    value_cache,
    lambdas,
    head_gain,
    out_weight,
    mixer_gain,
    gate_weight,
    up_weight,
    down_weight,
):
    batch = hidden_in.shape[0]
    n_tp = lax.axis_size(TP)
    n_kv = lax.axis_size(KV)
    own = hidden_in.astype(jnp.float32)
    first = to_all(jnp.concatenate([own, mixer_gain[None]], axis=0), TP)
    first = jnp.moveaxis(first, 0, 1).reshape(batch + 1, -1)
    block_f, mix_gain = first[:batch], first[batch:]
    gained = (block_f * attn_gain).astype(jnp.bfloat16)
    partial = jnp.dot(gained, query_weight, preferred_element_type=jnp.float32)
    heads = partial.shape[1] // LANES
    squares = jnp.sum(block_f * block_f, axis=1)
    packed = jnp.concatenate(
        [
            jnp.moveaxis(partial.reshape(batch, heads, LANES), 1, 0).reshape(-1, LANES),
            jnp.pad(squares[None], ((0, 7), (0, LANES - batch))),
        ],
        axis=0,
    )
    summed = to_all(packed, KV).sum(axis=0)
    inv = lax.rsqrt(summed[heads * batch, :batch] / D + eps)
    query = (
        summed[: heads * batch].reshape(heads, batch, LANES) * inv[None, :, None]
    ).astype(jnp.bfloat16)
    half = lax.broadcasted_iota(jnp.int32, (2, 1, 1, LANES), 3) // HEAD_DIM
    which = lax.broadcasted_iota(jnp.int32, (2, 1, 1, LANES), 0)
    split = jnp.where(half == which, query[None], jnp.zeros((), jnp.bfloat16))
    split = jnp.transpose(split, (2, 0, 1, 3)).reshape(batch, 2 * heads, LANES)
    positions = key_cache.shape[1]
    keys = key_cache.reshape(batch, positions, LANES)
    values = value_cache.reshape(batch, positions, LANES)
    scores = jnp.einsum(
        "brd,bpd->brp", split, keys, preferred_element_type=jnp.float32
    ) * HEAD_DIM ** (-0.5)
    maxima = jnp.max(scores, axis=-1)
    exponent = jnp.exp(scores - maxima[..., None])
    totals = jnp.sum(exponent, axis=-1)
    weighted = jnp.einsum(
        "brp,bpv->brv",
        exponent.astype(jnp.bfloat16),
        values,
        preferred_element_type=jnp.float32,
    )
    state = (maxima, totals, weighted)
    rows = batch * 2 * heads
    for axis in KV[::-1]:
        pack = jnp.concatenate(
            [
                state[2].reshape(rows, LANES),
                state[0].reshape(-1, LANES),
                state[1].reshape(-1, LANES),
                jnp.zeros((8 - 2 * rows // LANES, LANES), jnp.float32),
            ],
            axis=0,
        )
        parts = [state]
        k = rows // LANES
        for got in peers(pack, axis):
            parts.append(
                (
                    got[rows : rows + k].reshape(maxima.shape),
                    got[rows + k : rows + 2 * k].reshape(maxima.shape),
                    got[:rows].reshape(weighted.shape),
                )
            )
        state = merged(parts)
    means = (state[2] / state[1][..., None]).reshape(batch, 2, heads, LANES)
    attended = means[:, 0] - lambdas[None, :, None] * means[:, 1]
    norm = lax.rsqrt(jnp.mean(attended * attended, axis=-1, keepdims=True) + eps)
    head_out = (attended * norm * head_gain).astype(jnp.bfloat16).reshape(batch, -1)
    projected = jnp.dot(head_out, out_weight, preferred_element_type=jnp.float32)
    attn_out = to_all(projected.astype(jnp.bfloat16), TP).astype(jnp.float32).sum(axis=0)
    after_attn = (block_f + attn_out).astype(jnp.bfloat16)
    after_f = after_attn.astype(jnp.float32)
    squares_two = jnp.sum(after_f * after_f, axis=1, keepdims=True)
    mixer_in = (after_f * mix_gain).astype(jnp.bfloat16)
    gate_part = jnp.dot(mixer_in, gate_weight, preferred_element_type=jnp.float32)
    up_part = jnp.dot(mixer_in, up_weight, preferred_element_type=jnp.float32)
    width = gate_part.shape[1]
    both = jnp.concatenate(
        [gate_part, up_part, jnp.broadcast_to(squares_two, (batch, LANES))], axis=1
    ).reshape(batch, -1, LANES)
    row = lax.all_to_all(both, KV, 0, 0, tiled=True).sum(axis=0)
    k = width // LANES
    inv_two = lax.rsqrt(row[2 * k :, :] / D + eps)
    gate_sum, up_sum = row[:k] * inv_two, row[k : 2 * k] * inv_two
    hidden_share = (jax.nn.silu(gate_sum) * up_sum).astype(jnp.bfloat16)
    hidden = to_all(hidden_share, KV).reshape(batch, width)
    down_part = jnp.dot(hidden, down_weight, preferred_element_type=jnp.float32)
    tiles = jnp.moveaxis(down_part.astype(jnp.bfloat16).reshape(batch, n_tp, -1), 1, 0)
    arrived = lax.all_to_all(tiles, TP, 0, 0, tiled=True)
    mixer_out = arrived.astype(jnp.float32).sum(axis=0)
    cols = own.shape[1]
    mine = lax.dynamic_slice_in_dim(after_f, lax.axis_index(TP) * cols, cols, 1)
    return (mine + mixer_out).astype(jnp.bfloat16)


def solution(mesh):
    split = Mesh(mesh.devices.reshape(4, 4, 4, 2), ("kv_0", "kv_1", "tp_0", "tp_1"))
    placed = (
        P(None, KV_TP),
        P(KV),
        P(KV, TP),
        P(None, KV, TP, None),
        P(None, KV, TP, None),
        P(TP),
        P(),
        P(TP, KV),
        P(KV_TP),
        P(KV, TP),
        P(KV, TP),
        P(TP, KV),
    )
    return jax.shard_map(
        per_device, mesh=split, in_specs=placed, out_specs=P(None, KV_TP), check_vma=False
    )
```

```python
import jax
import jax.numpy as jnp
from jax import lax
from jax.sharding import Mesh
from jax.sharding import PartitionSpec as P

D = 4096
HEAD_DIM = 64
TP = ("tp_0", "tp_1")
KV = ("kv_0", "kv_1")
KV_TP = ("kv_0", "kv_1", "tp_0", "tp_1")
LANES = 128

eps = 1e-06


def to_all(shard, axis):
    length = lax.axis_size(axis)
    return lax.all_to_all(
        jnp.broadcast_to(shard[None], (length, *shard.shape)), axis, 0, 0, tiled=True
    )


def peers(shard, axis):
    n = lax.axis_size(axis)
    near = [1, 3, 2] if n == 4 else list(range(1, n))
    return [lax.ppermute(shard, axis, [(i, i ^ s) for i in range(n)]) for s in near]


def added(own, got):
    for p in got:
        own = own + p
    return own


def merged(parts):
    tops = [p[0] for p in parts]
    top = tops[0]
    for t in tops[1:]:
        top = jnp.maximum(top, t)
    total, acc = 0.0, 0.0
    for m, t, a in parts:
        f = jnp.exp(m - top)
        total = total + t * f
        acc = acc + a * f[..., None]
    return top, total, acc


def per_device(
    hidden_in,
    attn_gain,
    query_weight,
    key_cache,
    value_cache,
    lambdas,
    head_gain,
    out_weight,
    mixer_gain,
    gate_weight,
    up_weight,
    down_weight,
):
    batch = hidden_in.shape[0]
    n_tp = lax.axis_size(TP)
    own = hidden_in.astype(jnp.float32)
    first = to_all(jnp.concatenate([own, mixer_gain[None]], axis=0), TP)
    first = jnp.moveaxis(first, 0, 1).reshape(batch + 1, -1)
    block_f, mix_gain = first[:batch], first[batch:]
    gained = (block_f * attn_gain).astype(jnp.bfloat16)
    partial = jnp.dot(gained, query_weight, preferred_element_type=jnp.float32)
    width_q = partial.shape[1]
    heads = width_q // LANES
    squares = jnp.sum(block_f * block_f, axis=1, keepdims=True)
    packed = jnp.concatenate([partial, jnp.broadcast_to(squares, (batch, LANES))], axis=1)
    for axis in KV[::-1]:
        packed = added(packed, peers(packed, axis))
    inv = lax.rsqrt(packed[:, width_q : width_q + 1] / D + eps)
    query = (packed[:, :width_q] * inv).astype(jnp.bfloat16)
    query = jnp.moveaxis(query.reshape(batch, heads, LANES), 1, 0)
    half = lax.broadcasted_iota(jnp.int32, (2, 1, 1, LANES), 3) // HEAD_DIM
    which = lax.broadcasted_iota(jnp.int32, (2, 1, 1, LANES), 0)
    split = jnp.where(half == which, query[None], jnp.zeros((), jnp.bfloat16))
    split = jnp.transpose(split, (2, 0, 1, 3)).reshape(batch, 2 * heads, LANES)
    positions = key_cache.shape[1]
    keys = key_cache.reshape(batch, positions, LANES)
    values = value_cache.reshape(batch, positions, LANES)
    scores = jnp.einsum(
        "brd,bpd->brp", split, keys, preferred_element_type=jnp.float32
    ) * HEAD_DIM ** (-0.5)
    maxima = jnp.max(scores, axis=-1)
    exponent = jnp.exp(scores - maxima[..., None])
    totals = jnp.sum(exponent, axis=-1)
    weighted = jnp.einsum(
        "brp,bpv->brv",
        exponent.astype(jnp.bfloat16),
        values,
        preferred_element_type=jnp.float32,
    )
    state = (maxima, totals, weighted)
    rows = batch * 2 * heads
    for axis in KV[::-1]:
        pack = jnp.concatenate(
            [
                state[2].reshape(rows, LANES),
                state[0].reshape(-1, LANES),
                state[1].reshape(-1, LANES),
                jnp.zeros((8 - 2 * rows // LANES, LANES), jnp.float32),
            ],
            axis=0,
        )
        parts = [state]
        k = rows // LANES
        for got in peers(pack, axis):
            parts.append(
                (
                    got[rows : rows + k].reshape(maxima.shape),
                    got[rows + k : rows + 2 * k].reshape(maxima.shape),
                    got[:rows].reshape(weighted.shape),
                )
            )
        state = merged(parts)
    means = (state[2] / state[1][..., None]).reshape(batch, 2, heads, LANES)
    attended = means[:, 0] - lambdas[None, :, None] * means[:, 1]
    norm = lax.rsqrt(jnp.mean(attended * attended, axis=-1, keepdims=True) + eps)
    head_out = (attended * norm * head_gain).astype(jnp.bfloat16).reshape(batch, -1)
    projected = jnp.dot(head_out, out_weight, preferred_element_type=jnp.float32)
    attn_out = to_all(projected.astype(jnp.bfloat16), TP).astype(jnp.float32).sum(axis=0)
    after_attn = (block_f + attn_out).astype(jnp.bfloat16)
    after_f = after_attn.astype(jnp.float32)
    squares_two = jnp.sum(after_f * after_f, axis=1, keepdims=True)
    mixer_in = (after_f * mix_gain).astype(jnp.bfloat16)
    gate_part = jnp.dot(mixer_in, gate_weight, preferred_element_type=jnp.float32)
    up_part = jnp.dot(mixer_in, up_weight, preferred_element_type=jnp.float32)
    width = gate_part.shape[1]
    both = jnp.concatenate([gate_part, up_part], axis=1)
    lane = lax.broadcasted_iota(jnp.int32, (batch, LANES), 1)
    for axis in KV[::-1]:
        head = lax.reduce_precision(squares_two, 8, 7)
        tail = jnp.where(lane < LANES // 2, head, squares_two - head)
        sent = jnp.concatenate([both, tail], axis=1).astype(jnp.bfloat16)
        got = [p.astype(jnp.float32) for p in peers(sent, axis)]
        both = added(both, [p[:, : 2 * width] for p in got])
        squares_two = added(
            squares_two, [p[:, 2 * width : 2 * width + 1] + p[:, -1:] for p in got]
        )
    inv_two = lax.rsqrt(squares_two / D + eps)
    gate_sum, up_sum = both[:, :width] * inv_two, both[:, width:] * inv_two
    hidden = (jax.nn.silu(gate_sum) * up_sum).astype(jnp.bfloat16)
    down_part = jnp.dot(hidden, down_weight, preferred_element_type=jnp.float32)
    tiles = jnp.moveaxis(down_part.astype(jnp.bfloat16).reshape(batch, n_tp, -1), 1, 0)
    arrived = lax.all_to_all(tiles, TP, 0, 0, tiled=True)
    mixer_out = arrived.astype(jnp.float32).sum(axis=0)
    cols = own.shape[1]
    mine = lax.dynamic_slice_in_dim(after_f, lax.axis_index(TP) * cols, cols, 1)
    return (mine + mixer_out).astype(jnp.bfloat16)


def solution(mesh):
    split = Mesh(mesh.devices.reshape(4, 4, 4, 2), ("kv_0", "kv_1", "tp_0", "tp_1"))
    placed = (
        P(None, KV_TP),
        P(KV),
        P(KV, TP),
        P(None, KV, TP, None),
        P(None, KV, TP, None),
        P(TP),
        P(),
        P(TP, KV),
        P(KV_TP),
        P(KV, TP),
        P(KV, TP),
        P(TP, KV),
    )
    return jax.shard_map(
        per_device, mesh=split, in_specs=placed, out_specs=P(None, KV_TP), check_vma=False
    )
```

```python
import jax
import jax.numpy as jnp
from jax import lax
from jax.sharding import Mesh
from jax.sharding import PartitionSpec as P


D = 4096
HEAD_DIM = 64
TP = ("tp_0", "tp_1")
KV = ("kv_0", "kv_1")
KV_TP = ("kv_0", "kv_1", "tp_0", "tp_1")
LANES = 128

eps = 1e-06


def to_all(shard, axis):
    length = lax.axis_size(axis)
    return lax.all_to_all(
        jnp.broadcast_to(shard[None], (length, *shard.shape)), axis, 0, 0, tiled=True
    )


SHIFTS = (2, 3, 1)


def peers(shard, axis):
    n = lax.axis_size(axis)
    got = []
    for s in SHIFTS:
        got.append(lax.ppermute(shard, axis, [(i, i ^ s) for i in range(n)]))
    return got


def added(own, got):
    for p in got:
        own = own + p
    return own


def merged(parts):
    tops = [p[0] for p in parts]
    top = tops[0]
    for t in tops[1:]:
        top = jnp.maximum(top, t)
    total, acc = 0.0, 0.0
    for m, t, a in parts:
        f = jnp.exp(m - top)
        total = total + t * f
        acc = acc + a * f[..., None]
    return top, total, acc


def per_device(
    hidden_in,
    attn_gain,
    query_weight,
    key_cache,
    value_cache,
    lambdas,
    head_gain,
    out_weight,
    mixer_gain,
    gate_weight,
    up_weight,
    down_weight,
):
    batch = hidden_in.shape[0]
    n_tp = lax.axis_size(TP)
    own = hidden_in.astype(jnp.float32)
    first = to_all(jnp.concatenate([own, mixer_gain[None]], axis=0), TP)
    first = jnp.moveaxis(first, 0, 1).reshape(batch + 1, -1)
    block_f, mix_gain = first[:batch], first[batch:]
    gained = (block_f * attn_gain).astype(jnp.bfloat16)
    partial = jnp.dot(gained, query_weight, preferred_element_type=jnp.float32)
    width_q = partial.shape[1]
    heads = width_q // LANES
    squares = jnp.sum(block_f * block_f, axis=1, keepdims=True)
    packed = jnp.concatenate([partial, jnp.broadcast_to(squares, (batch, LANES))], axis=1)
    for axis in KV[::-1]:
        packed = added(packed, peers(packed, axis))
    inv = lax.rsqrt(packed[:, width_q : width_q + 1] / D + eps)
    query = (packed[:, :width_q] * inv).astype(jnp.bfloat16)
    query = jnp.moveaxis(query.reshape(batch, heads, LANES), 1, 0)
    half = lax.broadcasted_iota(jnp.int32, (2, 1, 1, LANES), 3) // HEAD_DIM
    which = lax.broadcasted_iota(jnp.int32, (2, 1, 1, LANES), 0)
    split = jnp.where(half == which, query[None], jnp.zeros((), jnp.bfloat16))
    split = jnp.transpose(split, (2, 0, 1, 3)).reshape(batch, 2 * heads, LANES)
    positions = key_cache.shape[1]
    keys = key_cache.reshape(batch, positions, LANES)
    values = value_cache.reshape(batch, positions, LANES)
    scores = jnp.einsum(
        "brd,bpd->brp", split, keys, preferred_element_type=jnp.float32
    ) * HEAD_DIM ** (-0.5)
    maxima = jnp.max(scores, axis=-1)
    exponent = jnp.exp(scores - maxima[..., None])
    totals = jnp.sum(exponent, axis=-1)
    weighted = jnp.einsum(
        "brp,bpv->brv",
        exponent.astype(jnp.bfloat16),
        values,
        preferred_element_type=jnp.float32,
    )
    state = (maxima, totals, weighted)
    rows = batch * 2 * heads
    for axis in KV[::-1]:
        pack = jnp.concatenate(
            [
                state[2].reshape(rows, LANES),
                state[0].reshape(-1, LANES),
                state[1].reshape(-1, LANES),
                jnp.zeros((8 - 2 * rows // LANES, LANES), jnp.float32),
            ],
            axis=0,
        )
        parts = [state]
        k = rows // LANES
        for got in peers(pack, axis):
            parts.append(
                (
                    got[rows : rows + k].reshape(maxima.shape),
                    got[rows + k : rows + 2 * k].reshape(maxima.shape),
                    got[:rows].reshape(weighted.shape),
                )
            )
        state = merged(parts)
    means = (state[2] / state[1][..., None]).reshape(batch, 2, heads, LANES)
    attended = means[:, 0] - lambdas[None, :, None] * means[:, 1]
    norm = lax.rsqrt(jnp.mean(attended * attended, axis=-1, keepdims=True) + eps)
    head_out = (attended * norm * head_gain).astype(jnp.bfloat16).reshape(batch, -1)
    projected = jnp.dot(head_out, out_weight, preferred_element_type=jnp.float32)
    attn_out = to_all(projected.astype(jnp.bfloat16), TP).astype(jnp.float32).sum(axis=0)
    after_attn = (block_f + attn_out).astype(jnp.bfloat16)
    after_f = after_attn.astype(jnp.float32)
    squares_two = jnp.sum(after_f * after_f, axis=1, keepdims=True)
    mixer_in = (after_f * mix_gain).astype(jnp.bfloat16)
    gate_part = jnp.dot(mixer_in, gate_weight, preferred_element_type=jnp.float32)
    up_part = jnp.dot(mixer_in, up_weight, preferred_element_type=jnp.float32)
    width = gate_part.shape[1]
    both = jnp.concatenate([gate_part, up_part], axis=1)
    lane = lax.broadcasted_iota(jnp.int32, (batch, LANES), 1)
    for axis in KV[::-1]:
        head = lax.reduce_precision(squares_two, 8, 7)
        tail = jnp.where(lane < LANES // 2, head, squares_two - head)
        sent = jnp.concatenate([both, tail], axis=1).astype(jnp.bfloat16)
        got = [p.astype(jnp.float32) for p in peers(sent, axis)]
        both = added(both, [p[:, : 2 * width] for p in got])
        squares_two = added(
            squares_two, [p[:, 2 * width : 2 * width + 1] + p[:, -1:] for p in got]
        )
    inv_two = lax.rsqrt(squares_two / D + eps)
    gate_sum, up_sum = both[:, :width] * inv_two, both[:, width:] * inv_two
    hidden = (jax.nn.silu(gate_sum) * up_sum).astype(jnp.bfloat16)
    down_part = jnp.dot(hidden, down_weight, preferred_element_type=jnp.float32)
    tiles = jnp.moveaxis(down_part.astype(jnp.bfloat16).reshape(batch, n_tp, -1), 1, 0)
    arrived = lax.all_to_all(tiles, TP, 0, 0, tiled=True)
    mixer_out = arrived.astype(jnp.float32).sum(axis=0)
    cols = own.shape[1]
    mine = lax.dynamic_slice_in_dim(after_f, lax.axis_index(TP) * cols, cols, 1)
    return (mine + mixer_out).astype(jnp.bfloat16)


def solution(mesh):
    split = Mesh(mesh.devices.reshape(4, 4, 4, 2), ("kv_0", "kv_1", "tp_0", "tp_1"))
    placed = (
        P(None, KV_TP),
        P(KV),
        P(KV, TP),
        P(None, KV, TP, None),
        P(None, KV, TP, None),
        P(TP),
        P(),
        P(TP, KV),
        P(KV_TP),
        P(KV, TP),
        P(KV, TP),
        P(TP, KV),
    )
    return jax.shard_map(
        per_device, mesh=split, in_specs=placed, out_specs=P(None, KV_TP), check_vma=False
    )
```

```python
import functools

import jax
import jax.numpy as jnp
from jax import lax
from jax.experimental import pallas as pl
from jax.experimental.pallas import tpu as pltpu
from jax.sharding import Mesh
from jax.sharding import PartitionSpec as P


D = 4096
HEAD_DIM = 64
KV = ("kv_0", "kv_1")
KV_TP = ("kv_0", "kv_1", "tp_0", "tp_1")
TP = ("tp_0", "tp_1")
LANES = 128
F32 = jnp.float32
BF16 = jnp.bfloat16

eps = 1e-06

SHIFTS = (2, 3, 1)


def peers(shard, axis):
    n = lax.axis_size(axis)
    got = []
    for s in SHIFTS:
        got.append(lax.ppermute(shard, axis, [(i, i ^ s) for i in range(n)]))
    return got


def partner(shard):
    return lax.ppermute(shard, TP[1], [(0, 1), (1, 0)])


def added(own, got):
    for p in got:
        own = own + p
    return own


def lane_of(shape):
    return lax.broadcasted_iota(jnp.int32, shape, len(shape) - 1)


def kernel_call(body, outs, scratch=(), smem=0, n_in=1, mib=16):
    spec = [pl.BlockSpec(memory_space=pltpu.SMEM)] * smem
    spec += [pl.BlockSpec(memory_space=pltpu.VMEM)] * (n_in - smem)
    return pl.pallas_call(
        body,
        out_shape=outs,
        in_specs=spec,
        out_specs=[pl.BlockSpec(memory_space=pltpu.VMEM)] * len(outs),
        scratch_shapes=scratch,
        compiler_params=pltpu.CompilerParams(vmem_limit_bytes=mib * 2**20),
    )


def query_body(chip, own, a, b, c, gain, weight, packed, block, held):
    batch = packed.shape[0]
    x = chip[0]
    held[x] = own[...]
    for s, ref in zip(SHIFTS, (a, b, c)):
        held[x ^ s] = ref[...]
    left = lane_of(own.shape) < LANES // 2
    for t in range(2):
        block[:, t * LANES : (t + 1) * LANES] = jnp.where(left, held[2 * t], held[2 * t + 1])
    rows = block[:batch, :]
    gained = (rows * gain[...]).astype(BF16)
    width = weight.shape[1]
    packed[:, :width] = jnp.dot(gained, weight[...], preferred_element_type=F32)
    squares = jnp.sum(rows * rows, axis=1, keepdims=True)
    packed[:, width:] = jnp.broadcast_to(squares, (batch, LANES))


def attend_body(own, a, b, c, keys, values, out, query):
    batch, _, _ = keys.shape
    width = own.shape[1] - LANES
    heads = width // LANES
    whole = own[...] + a[...] + b[...] + c[...]
    inv = lax.rsqrt(whole[:, width:] / D + eps)
    for g in range(heads):
        part = whole[:, g * LANES : (g + 1) * LANES] * inv
        query[g * batch : (g + 1) * batch, :] = part.astype(BF16).astype(F32)
    shape = (2 * heads, LANES)
    half = lane_of(shape) // HEAD_DIM
    keep = half == lax.broadcasted_iota(jnp.int32, shape, 0) // heads
    lane = lane_of(shape)
    stats = jnp.zeros(shape, F32)
    for n in range(batch):
        q = query[pl.ds(n, heads, stride=batch), :]
        q = jnp.where(keep, jnp.concatenate([q, q], axis=0), 0.0).astype(BF16)
        scores = lax.dot_general(
            q, keys[n], (((1,), (1,)), ((), ())), preferred_element_type=F32
        ) * HEAD_DIM ** (-0.5)
        top = jnp.max(scores, axis=1, keepdims=True)
        exponent = jnp.exp(scores - top)
        total = jnp.sum(exponent, axis=1, keepdims=True)
        out[n * 2 * heads : (n + 1) * 2 * heads, :] = jnp.dot(
            exponent.astype(BF16), values[n], preferred_element_type=F32
        )
        stats = jnp.where(lane == n, top, stats)
        stats = jnp.where(lane == n + LANES // 2, total, stats)
    out[batch * 2 * heads :, :] = stats


def combined(parts, rows, high):
    n = rows * high
    stats = [p[n : n + high, :] for p in parts]
    top = functools.reduce(jnp.maximum, stats)
    factors = [jnp.exp(s - top) for s in stats]
    shifted = [pltpu.roll(f, LANES // 2, 1) for f in factors]
    total = sum(s * f for s, f in zip(stats, shifted))
    low = lane_of(top.shape) < LANES // 2
    accs = []
    for k in range(rows):
        acc = 0.0
        for p, f in zip(parts, factors):
            acc = acc + p[k * high : (k + 1) * high, :] * f[:, k : k + 1]
        accs.append(acc)
    return jnp.where(low, top, total), accs


def merge_body(own, a, b, c, out):
    high = 8
    rows = own.shape[0] // high - 1
    stats, accs = combined((own, a, b, c), rows, high)
    for k, acc in enumerate(accs):
        out[k * high : (k + 1) * high, :] = acc
    out[rows * high :, :] = stats


def project_body(lambdas, own, a, b, c, gain, weight, out, held):
    high = 8
    heads = high // 2
    rows = own.shape[0] // high - 1
    stats, accs = combined((own, a, b, c), rows, high)
    inverse = 1.0 / stats
    at = lax.broadcasted_iota(jnp.int32, (heads, LANES), 0)
    mixing = jnp.zeros((heads, LANES), F32)
    for g in range(heads):
        mixing = jnp.where(at == g, lambdas[g], mixing)
    for k, acc in enumerate(accs):
        at_lane = LANES // 2 + k
        means = acc * inverse[:, at_lane : at_lane + 1]
        attended = means[:heads] - mixing * means[heads:]
        norm = lax.rsqrt(jnp.mean(attended * attended, axis=1, keepdims=True) + eps)
        held[pl.ds(k, heads, stride=rows), :] = attended * norm * gain[...]
    projected = 0.0
    for g in range(heads):
        projected = projected + jnp.dot(
            held[g * rows : (g + 1) * rows, :].astype(BF16),
            weight[g * LANES : (g + 1) * LANES, :],
            preferred_element_type=F32,
        )
    out[...] = projected.astype(BF16)


def gate_body(attn, other, block, gate, up, both, sent, after):
    batch = attn.shape[0]
    rows = (block[:batch, :] + (attn[...] + other[...])).astype(BF16).astype(F32)
    after[...] = rows
    squares = jnp.sum(rows * rows, axis=1, keepdims=True)
    mixer_in = (rows * block[batch : batch + 1, :]).astype(BF16)
    width = gate.shape[1]
    for k, weight in enumerate((gate, up)):
        part = jnp.dot(mixer_in, weight[...], preferred_element_type=F32)
        both[:, k * width : (k + 1) * width] = part
        sent[:, k * width : (k + 1) * width] = part.astype(BF16)
    both[:, 2 * width :] = jnp.broadcast_to(squares, (batch, LANES))
    sent[:, 2 * width :] = high_and_low(squares, batch)


def high_and_low(squares, batch):
    high = squares.astype(BF16).astype(F32)
    low = lane_of((batch, LANES)) >= LANES // 2
    return jnp.where(low, squares - high, high).astype(BF16)


def gathered_sums(own, others):
    width = own.shape[1] - LANES
    sums = own[:, :width]
    squares = own[:, width : width + 1]
    for p in others:
        sums = sums + p[:, :width].astype(F32)
        tail = p[:, width:].astype(F32)
        squares = squares + (tail[:, :1] + tail[:, LANES // 2 : LANES // 2 + 1])
    return sums, squares


def middle_body(own, a, b, c, both, sent):
    sums, squares = gathered_sums(own, (a, b, c))
    batch, width = sums.shape
    both[:, :width] = sums
    sent[:, :width] = sums.astype(BF16)
    both[:, width:] = jnp.broadcast_to(squares, (batch, LANES))
    sent[:, width:] = high_and_low(squares, batch)


def down_body(own, a, b, c, weight, out):
    sums, squares = gathered_sums(own, (a, b, c))
    width = sums.shape[1] // 2
    inv = lax.rsqrt(squares / D + eps)
    gate, up = sums[:, :width] * inv, sums[:, width:] * inv
    hidden = (gate / (1.0 + jnp.exp(-gate)) * up).astype(BF16)
    out[...] = jnp.dot(hidden, weight[...], preferred_element_type=F32).astype(BF16)


def per_device(
    hidden_in,
    attn_gain,
    query_weight,
    key_cache,
    value_cache,
    lambdas,
    head_gain,
    out_weight,
    mixer_gain,
    gate_weight,
    up_weight,
    down_weight,
):
    batch, cols = hidden_in.shape
    width_q = query_weight.shape[1]
    heads = width_q // LANES
    wide = query_weight.shape[0]
    positions = key_cache.shape[1]
    shape = jax.ShapeDtypeStruct
    core = lax.axis_index(TP[1])
    chip = lax.axis_index(TP[0]).astype(jnp.int32)

    own = jnp.concatenate([hidden_in.astype(F32), mixer_gain[None]], axis=0)
    own = jnp.concatenate([own] * (LANES // cols), axis=1)
    own = jnp.pad(own, ((0, 7), (0, 0)))
    mine = lane_of(own.shape) // cols % 2 == core
    pair = jnp.where(mine, own, partner(own))
    packed, block = kernel_call(
        query_body,
        [shape((batch, width_q + LANES), F32), shape((own.shape[0], wide), F32)],
        [pltpu.VMEM((4, *own.shape), F32)],
        smem=1,
        n_in=7,
    )(chip[None], pair, *peers(pair, "tp_0"), attn_gain[None], query_weight)
    packed = added(packed, peers(packed, "kv_1"))
    state = kernel_call(
        attend_body,
        [shape(((batch + 1) * 2 * heads, LANES), F32)],
        [pltpu.VMEM((heads * batch, LANES), F32)],
        n_in=6,
    )(
        packed,
        *peers(packed, "kv_0"),
        key_cache.reshape(batch, positions, LANES),
        value_cache.reshape(batch, positions, LANES),
    )[0]
    state = kernel_call(merge_body, [shape(state.shape, F32)], n_in=4)(
        state, *peers(state, "kv_1")
    )[0]
    projected = kernel_call(
        project_body,
        [shape((batch, wide), BF16)],
        [pltpu.VMEM((heads * batch, LANES), F32)],
        smem=1,
        n_in=7,
    )(lambdas, state, *peers(state, "kv_0"), head_gain[None], out_weight)[0]
    attn = added(
        projected.astype(F32), [p.astype(F32) for p in peers(projected, "tp_0")]
    )
    width = gate_weight.shape[1]
    both_shape = (batch, 2 * width + LANES)
    both, sent, after = kernel_call(
        gate_body,
        [shape(both_shape, F32), shape(both_shape, BF16), shape((batch, wide), F32)],
        n_in=5,
    )(attn, partner(attn), block, gate_weight, up_weight)
    both, sent = kernel_call(
        middle_body, [shape(both_shape, F32), shape(both_shape, BF16)], n_in=4
    )(both, *peers(sent, "kv_1"))
    down = kernel_call(down_body, [shape((batch, wide), BF16)], n_in=5)(
        both, *peers(sent, "kv_0"), down_weight
    )[0]
    mix = added(down.astype(F32), [p.astype(F32) for p in peers(down, "tp_0")])
    mixed = after + (mix + partner(mix))
    return lax.dynamic_slice_in_dim(mixed, (chip * 2 + core) * cols, cols, 1).astype(BF16)


def solution(mesh):
    split = Mesh(mesh.devices.reshape(4, 4, 4, 2), ("kv_0", "kv_1", "tp_0", "tp_1"))
    placed = (
        P(None, KV_TP),
        P(KV),
        P(KV, TP),
        P(None, KV, TP, None),
        P(None, KV, TP, None),
        P(TP),
        P(),
        P(TP, KV),
        P(KV_TP),
        P(KV, TP),
        P(KV, TP),
        P(TP, KV),
    )
    return jax.shard_map(
        per_device, mesh=split, in_specs=placed, out_specs=P(None, KV_TP), check_vma=False
    )
```

```python
import functools

import jax
import jax.numpy as jnp
from jax import lax
from jax.experimental import pallas as pl
from jax.experimental.pallas import tpu as pltpu
from jax.sharding import Mesh
from jax.sharding import PartitionSpec as P


D = 4096
HEAD_DIM = 64
KV = ("kv_0", "kv_1")
KV_TP = ("kv_0", "kv_1", "tp_0", "tp_1")
TP = ("tp_0", "tp_1")
LANES = 128
F32 = jnp.float32
BF16 = jnp.bfloat16

eps = 1e-06
COST = 2**40

SHIFTS = (2, 3, 1)


def peers(shard, axis):
    n = lax.axis_size(axis)
    got = []
    for s in SHIFTS:
        got.append(lax.ppermute(shard, axis, [(i, i ^ s) for i in range(n)]))
    return got


def partner(shard):
    return lax.ppermute(shard, TP[1], [(0, 1), (1, 0)])


def added(own, got):
    for p in got:
        own = own + p
    return own


def lane_of(shape):
    return lax.broadcasted_iota(jnp.int32, shape, len(shape) - 1)


def kernel_call(body, outs, scratch=(), smem=0, n_in=1, mib=16, cost=0):
    spec = [pl.BlockSpec(memory_space=pltpu.SMEM)] * smem
    spec += [pl.BlockSpec(memory_space=pltpu.VMEM)] * (n_in - smem)
    return pl.pallas_call(
        body,
        out_shape=outs,
        in_specs=spec,
        out_specs=[pl.BlockSpec(memory_space=pltpu.VMEM)] * len(outs),
        scratch_shapes=scratch,
        compiler_params=pltpu.CompilerParams(vmem_limit_bytes=mib * 2**20),
        cost_estimate=pl.CostEstimate(flops=cost, bytes_accessed=cost, transcendentals=0)
        if cost
        else None,
    )


def pack_body(hidden, gain, out, rows, scale, sems):
    loads = [
        pltpu.make_async_copy(hidden, rows, sems.at[0]),
        pltpu.make_async_copy(gain, scale, sems.at[1]),
    ]
    for load in loads:
        load.start()
    for load in loads:
        load.wait()
    batch, cols = hidden.shape
    out[:batch, :] = jnp.concatenate([rows[...].astype(F32)] * (LANES // cols), axis=1)
    row = jnp.concatenate([scale[...]] * (LANES // cols), axis=1)
    out[batch:, :] = jnp.broadcast_to(row, (out.shape[0] - batch, LANES))


def query_body(chip, own, a, b, c, gain, weight, packed, block, held):
    batch = packed.shape[0]
    x = chip[0]
    held[x] = own[...]
    for s, ref in zip(SHIFTS, (a, b, c)):
        held[x ^ s] = ref[...]
    left = lane_of(own.shape) < LANES // 2
    for t in range(2):
        block[:, t * LANES : (t + 1) * LANES] = jnp.where(left, held[2 * t], held[2 * t + 1])
    rows = block[:batch, :]
    gained = (rows * gain[...]).astype(BF16)
    width = weight.shape[1]
    packed[:, :width] = jnp.dot(gained, weight[...], preferred_element_type=F32)
    squares = jnp.sum(rows * rows, axis=1, keepdims=True)
    packed[:, width:] = jnp.broadcast_to(squares, (batch, LANES))


def attend_body(own, a, b, c, keys, values, out, query, scores, weights):
    batch, _, _ = keys.shape
    width = own.shape[1] - LANES
    heads = width // LANES
    whole = own[...] + a[...] + b[...] + c[...]
    inv = lax.rsqrt(whole[:, width:] / D + eps)
    for g in range(heads):
        part = whole[:, g * LANES : (g + 1) * LANES] * inv
        query[g * batch : (g + 1) * batch, :] = part.astype(BF16).astype(F32)
    shape = (2 * heads, LANES)
    half = lane_of(shape) // HEAD_DIM
    keep = half == lax.broadcasted_iota(jnp.int32, shape, 0) // heads
    lane = lane_of(shape)
    high = 2 * heads
    for n in range(batch):
        q = query[pl.ds(n, heads, stride=batch), :]
        q = jnp.where(keep, jnp.concatenate([q, q], axis=0), 0.0).astype(BF16)
        scores[n * high : (n + 1) * high, :] = lax.dot_general(
            q, keys[n], (((1,), (1,)), ((), ())), preferred_element_type=F32
        )
    stats = jnp.zeros(shape, F32)
    for n in range(batch):
        score = scores[n * high : (n + 1) * high, :] * HEAD_DIM ** (-0.5)
        top = jnp.max(score, axis=1, keepdims=True)
        exponent = jnp.exp(score - top)
        total = jnp.sum(exponent, axis=1, keepdims=True)
        weights[n] = exponent.astype(BF16)
        stats = jnp.where(lane == n, top, stats)
        stats = jnp.where(lane == n + LANES // 2, total, stats)
    out[batch * high :, :] = stats
    for n in range(batch):
        out[n * high : (n + 1) * high, :] = jnp.dot(
            weights[n], values[n], preferred_element_type=F32
        )


def combined(parts, rows, high):
    n = rows * high
    stats = [p[n : n + high, :] for p in parts]
    top = functools.reduce(jnp.maximum, stats)
    factors = [jnp.exp(s - top) for s in stats]
    shifted = [pltpu.roll(f, LANES // 2, 1) for f in factors]
    total = sum(s * f for s, f in zip(stats, shifted))
    low = lane_of(top.shape) < LANES // 2
    accs = []
    for k in range(rows):
        acc = 0.0
        for p, f in zip(parts, factors):
            acc = acc + p[k * high : (k + 1) * high, :] * f[:, k : k + 1]
        accs.append(acc)
    return jnp.where(low, top, total), accs


def merge_body(own, a, b, c, out):
    high = 8
    rows = own.shape[0] // high - 1
    stats, accs = combined((own, a, b, c), rows, high)
    for k, acc in enumerate(accs):
        out[k * high : (k + 1) * high, :] = acc
    out[rows * high :, :] = stats


def project_body(lambdas, own, a, b, c, gain, weight, out, held):
    high = 8
    heads = high // 2
    rows = own.shape[0] // high - 1
    stats, accs = combined((own, a, b, c), rows, high)
    inverse = 1.0 / stats
    for k, acc in enumerate(accs):
        at_lane = LANES // 2 + k
        held[k * high : (k + 1) * high, :] = acc * inverse[:, at_lane : at_lane + 1]
    projected = 0.0
    for g in range(heads):
        first = held[pl.ds(g, rows, stride=high), :]
        second = held[pl.ds(heads + g, rows, stride=high), :]
        attended = first - lambdas[:, g : g + 1] * second
        norm = lax.rsqrt(jnp.mean(attended * attended, axis=1, keepdims=True) + eps)
        projected = projected + jnp.dot(
            (attended * norm * gain[...]).astype(BF16),
            weight[g * LANES : (g + 1) * LANES, :],
            preferred_element_type=F32,
        )
    out[...] = projected.astype(BF16)


def gate_body(attn, other, block, gate, up, both, sent, after):
    batch = attn.shape[0]
    rows = (block[:batch, :] + (attn[...] + other[...])).astype(BF16).astype(F32)
    after[...] = rows
    squares = jnp.sum(rows * rows, axis=1, keepdims=True)
    mixer_in = (rows * block[batch : batch + 1, :]).astype(BF16)
    width = gate.shape[1]
    for k, weight in enumerate((gate, up)):
        part = jnp.dot(mixer_in, weight[...], preferred_element_type=F32)
        both[:, k * width : (k + 1) * width] = part
        sent[:, k * width : (k + 1) * width] = part.astype(BF16)
    both[:, 2 * width :] = jnp.broadcast_to(squares, (batch, LANES))
    sent[:, 2 * width :] = high_and_low(squares, batch)


def high_and_low(squares, batch):
    high = squares.astype(BF16).astype(F32)
    low = lane_of((batch, LANES)) >= LANES // 2
    return jnp.where(low, squares - high, high).astype(BF16)


def gathered_sums(own, others):
    width = own.shape[1] - LANES
    sums = own[:, :width]
    squares = own[:, width : width + 1]
    for p in others:
        sums = sums + p[:, :width].astype(F32)
        tail = p[:, width:].astype(F32)
        squares = squares + (tail[:, :1] + tail[:, LANES // 2 : LANES // 2 + 1])
    return sums, squares


def middle_body(own, a, b, c, both, sent):
    sums, squares = gathered_sums(own, (a, b, c))
    batch, width = sums.shape
    both[:, :width] = sums
    sent[:, :width] = sums.astype(BF16)
    both[:, width:] = jnp.broadcast_to(squares, (batch, LANES))
    sent[:, width:] = high_and_low(squares, batch)


def down_body(own, a, b, c, weight, out):
    sums, squares = gathered_sums(own, (a, b, c))
    width = sums.shape[1] // 2
    inv = lax.rsqrt(squares / D + eps)
    gate, up = sums[:, :width] * inv, sums[:, width:] * inv
    hidden = (gate / (1.0 + jnp.exp(-gate)) * up).astype(BF16)
    out[...] = jnp.dot(hidden, weight[...], preferred_element_type=F32).astype(BF16)


def per_device(
    hidden_in,
    attn_gain,
    query_weight,
    key_cache,
    value_cache,
    lambdas,
    head_gain,
    out_weight,
    mixer_gain,
    gate_weight,
    up_weight,
    down_weight,
):
    batch, cols = hidden_in.shape
    width_q = query_weight.shape[1]
    heads = width_q // LANES
    wide = query_weight.shape[0]
    positions = key_cache.shape[1]
    shape = jax.ShapeDtypeStruct
    core = lax.axis_index(TP[1])
    chip = lax.axis_index(TP[0]).astype(jnp.int32)

    own = pl.pallas_call(
        pack_body,
        out_shape=shape((batch + 8, LANES), F32),
        in_specs=[pl.BlockSpec(memory_space=pltpu.HBM)] * 2,
        out_specs=pl.BlockSpec(memory_space=pltpu.VMEM),
        scratch_shapes=[
            pltpu.VMEM((batch, cols), BF16),
            pltpu.VMEM((1, cols), F32),
            pltpu.SemaphoreType.DMA((2,)),
        ],
        compiler_params=pltpu.CompilerParams(vmem_limit_bytes=4 * 2**20),
        cost_estimate=pl.CostEstimate(flops=COST, bytes_accessed=COST, transcendentals=0),
    )(
        pltpu.with_memory_space_constraint(hidden_in, pltpu.HBM),
        pltpu.with_memory_space_constraint(mixer_gain[None], pltpu.HBM),
    )
    mine = lane_of(own.shape) // cols % 2 == core
    pair = jnp.where(mine, own, partner(own))
    packed, block = kernel_call(
        query_body,
        [shape((batch, width_q + LANES), F32), shape((own.shape[0], wide), F32)],
        [pltpu.VMEM((4, *own.shape), F32)],
        smem=1,
        n_in=7,
        cost=COST,
    )(chip[None], pair, *peers(pair, "tp_0"), attn_gain[None], query_weight)
    packed = added(packed, peers(packed, "kv_1"))
    state = kernel_call(
        attend_body,
        [shape(((batch + 1) * 2 * heads, LANES), F32)],
        [
            pltpu.VMEM((heads * batch, LANES), F32),
            pltpu.VMEM((2 * heads * batch, positions), F32),
            pltpu.VMEM((batch, 2 * heads, positions), BF16),
        ],
        n_in=6,
    )(
        packed,
        *peers(packed, "kv_0"),
        key_cache.reshape(batch, positions, LANES),
        value_cache.reshape(batch, positions, LANES),
    )[0]
    state = kernel_call(merge_body, [shape(state.shape, F32)], n_in=4)(
        state, *peers(state, "kv_1")
    )[0]
    projected = kernel_call(
        project_body,
        [shape((batch, wide), BF16)],
        [pltpu.VMEM((2 * heads * batch, LANES), F32)],
        n_in=7,
    )(lambdas[None], state, *peers(state, "kv_0"), head_gain[None], out_weight)[0]
    attn = added(
        projected.astype(F32), [p.astype(F32) for p in peers(projected, "tp_0")]
    )
    width = gate_weight.shape[1]
    both_shape = (batch, 2 * width + LANES)
    both, sent, after = kernel_call(
        gate_body,
        [shape(both_shape, F32), shape(both_shape, BF16), shape((batch, wide), F32)],
        n_in=5,
    )(attn, partner(attn), block, gate_weight, up_weight)
    both, sent = kernel_call(
        middle_body, [shape(both_shape, F32), shape(both_shape, BF16)], n_in=4
    )(both, *peers(sent, "kv_1"))
    down = kernel_call(down_body, [shape((batch, wide), BF16)], n_in=5)(
        both, *peers(sent, "kv_0"), down_weight
    )[0]
    mix = added(down.astype(F32), [p.astype(F32) for p in peers(down, "tp_0")])
    mixed = after + (mix + partner(mix))
    return lax.dynamic_slice_in_dim(mixed, (chip * 2 + core) * cols, cols, 1).astype(BF16)


def solution(mesh):
    split = Mesh(mesh.devices.reshape(4, 4, 4, 2), ("kv_0", "kv_1", "tp_0", "tp_1"))
    placed = (
        P(None, KV_TP),
        P(KV),
        P(KV, TP),
        P(None, KV, TP, None),
        P(None, KV, TP, None),
        P(TP),
        P(),
        P(TP, KV),
        P(KV_TP),
        P(KV, TP),
        P(KV, TP),
        P(TP, KV),
    )
    return jax.shard_map(
        per_device, mesh=split, in_specs=placed, out_specs=P(None, KV_TP), check_vma=False
    )
```

```python
import functools

import jax
import jax.numpy as jnp
from jax import lax
from jax.experimental import pallas as pl
from jax.experimental.pallas import tpu as pltpu
from jax.sharding import Mesh
from jax.sharding import PartitionSpec as P


D = 4096
HEAD_DIM = 64
KV = ("kv_0", "kv_1")
KV_TP = ("kv_0", "kv_1", "tp_0", "tp_1")
TP = ("tp_0", "tp_1")
LANES = 128
F32 = jnp.float32
BF16 = jnp.bfloat16

eps = 1e-06
COST = 2**40

SHIFTS = (2, 3, 1)
STRAIGHT = ("gates", "heads")


def peers(shard, axis, what):
    across, wide = (axis, 1) if what in STRAIGHT else ((axis, TP[1]), 2)
    n = lax.axis_size(across)
    got = []
    for s in SHIFTS:
        pairs = [(i, i ^ (wide * s + wide - 1)) for i in range(n)]
        got.append(lax.ppermute(shard, across, pairs))
    return got


def partner(shard):
    return lax.ppermute(shard, TP[1], [(0, 1), (1, 0)])


def added(own, got):
    for p in got:
        own = own + p
    return own


def lane_of(shape):
    return lax.broadcasted_iota(jnp.int32, shape, len(shape) - 1)


def kernel_call(body, outs, scratch=(), smem=0, n_in=1, mib=16, cost=0):
    spec = [pl.BlockSpec(memory_space=pltpu.SMEM)] * smem
    spec += [pl.BlockSpec(memory_space=pltpu.VMEM)] * (n_in - smem)
    return pl.pallas_call(
        body,
        out_shape=outs,
        in_specs=spec,
        out_specs=[pl.BlockSpec(memory_space=pltpu.VMEM)] * len(outs),
        scratch_shapes=scratch,
        compiler_params=pltpu.CompilerParams(vmem_limit_bytes=mib * 2**20),
        cost_estimate=pl.CostEstimate(flops=cost, bytes_accessed=cost, transcendentals=0)
        if cost
        else None,
    )


def pack_body(hidden, gain, out, rows, scale, sems):
    loads = [
        pltpu.make_async_copy(hidden, rows, sems.at[0]),
        pltpu.make_async_copy(gain, scale, sems.at[1]),
    ]
    for load in loads:
        load.start()
    for load in loads:
        load.wait()
    batch, cols = hidden.shape
    out[:batch, :] = jnp.concatenate([rows[...].astype(F32)] * (LANES // cols), axis=1)
    row = jnp.concatenate([scale[...]] * (LANES // cols), axis=1)
    out[batch:, :] = jnp.broadcast_to(row, (out.shape[0] - batch, LANES))


def query_body(chip, own, a, b, c, gain, weight, packed, block, held):
    batch = packed.shape[0]
    x = chip[0]
    held[x] = own[...]
    for s, ref in zip(SHIFTS, (a, b, c)):
        held[x ^ s] = ref[...]
    left = lane_of(own.shape) < LANES // 2
    for t in range(2):
        block[:, t * LANES : (t + 1) * LANES] = jnp.where(left, held[2 * t], held[2 * t + 1])
    rows = block[:batch, :]
    gained = (rows * gain[...]).astype(BF16)
    width = weight.shape[1]
    packed[:, :width] = jnp.dot(gained, weight[...], preferred_element_type=F32)
    squares = jnp.sum(rows * rows, axis=1, keepdims=True)
    packed[:, width:] = jnp.broadcast_to(squares, (batch, LANES))


def attend_body(own, a, b, c, keys, values, out, query, scores, weights):
    batch, _, _ = keys.shape
    width = own.shape[1] - LANES
    heads = width // LANES
    whole = own[...] + a[...] + b[...] + c[...]
    inv = lax.rsqrt(whole[:, width:] / D + eps)
    for g in range(heads):
        part = whole[:, g * LANES : (g + 1) * LANES] * inv
        query[g * batch : (g + 1) * batch, :] = part.astype(BF16).astype(F32)
    shape = (2 * heads, LANES)
    half = lane_of(shape) // HEAD_DIM
    keep = half == lax.broadcasted_iota(jnp.int32, shape, 0) // heads
    lane = lane_of(shape)
    high = 2 * heads
    for n in range(batch):
        q = query[pl.ds(n, heads, stride=batch), :]
        q = jnp.where(keep, jnp.concatenate([q, q], axis=0), 0.0).astype(BF16)
        scores[n * high : (n + 1) * high, :] = lax.dot_general(
            q, keys[n], (((1,), (1,)), ((), ())), preferred_element_type=F32
        )
    stats = jnp.zeros(shape, F32)
    for n in range(batch):
        score = scores[n * high : (n + 1) * high, :] * HEAD_DIM ** (-0.5)
        top = jnp.max(score, axis=1, keepdims=True)
        exponent = jnp.exp(score - top)
        total = jnp.sum(exponent, axis=1, keepdims=True)
        weights[n] = exponent.astype(BF16)
        stats = jnp.where(lane == n, top, stats)
        stats = jnp.where(lane == n + LANES // 2, total, stats)
    out[batch * high :, :] = stats
    for n in range(batch):
        out[n * high : (n + 1) * high, :] = jnp.dot(
            weights[n], values[n], preferred_element_type=F32
        )


def combined(parts, rows, high):
    n = rows * high
    stats = [p[n : n + high, :] for p in parts]
    top = functools.reduce(jnp.maximum, stats)
    factors = [jnp.exp(s - top) for s in stats]
    shifted = [pltpu.roll(f, LANES // 2, 1) for f in factors]
    total = sum(s * f for s, f in zip(stats, shifted))
    low = lane_of(top.shape) < LANES // 2
    accs = []
    for k in range(rows):
        acc = 0.0
        for p, f in zip(parts, factors):
            acc = acc + p[k * high : (k + 1) * high, :] * f[:, k : k + 1]
        accs.append(acc)
    return jnp.where(low, top, total), accs


def merge_body(own, a, b, c, out):
    high = 8
    rows = own.shape[0] // high - 1
    stats, accs = combined((own, a, b, c), rows, high)
    for k, acc in enumerate(accs):
        out[k * high : (k + 1) * high, :] = acc
    out[rows * high :, :] = stats


def project_body(lambdas, own, a, b, c, gain, weight, out, held):
    high = 8
    heads = high // 2
    rows = own.shape[0] // high - 1
    stats, accs = combined((own, a, b, c), rows, high)
    inverse = 1.0 / stats
    for k, acc in enumerate(accs):
        at_lane = LANES // 2 + k
        held[k * high : (k + 1) * high, :] = acc * inverse[:, at_lane : at_lane + 1]
    projected = 0.0
    for g in range(heads):
        first = held[pl.ds(g, rows, stride=high), :]
        second = held[pl.ds(heads + g, rows, stride=high), :]
        attended = first - lambdas[:, g : g + 1] * second
        norm = lax.rsqrt(jnp.mean(attended * attended, axis=1, keepdims=True) + eps)
        projected = projected + jnp.dot(
            (attended * norm * gain[...]).astype(BF16),
            weight[g * LANES : (g + 1) * LANES, :],
            preferred_element_type=F32,
        )
    out[...] = projected.astype(BF16)


def gate_body(attn, other, block, gate, up, both, sent, after):
    batch = attn.shape[0]
    rows = (block[:batch, :] + (attn[...] + other[...])).astype(BF16).astype(F32)
    after[...] = rows
    squares = jnp.sum(rows * rows, axis=1, keepdims=True)
    mixer_in = (rows * block[batch : batch + 1, :]).astype(BF16)
    width = gate.shape[1]
    for k, weight in enumerate((gate, up)):
        part = jnp.dot(mixer_in, weight[...], preferred_element_type=F32)
        both[:, k * width : (k + 1) * width] = part
        sent[:, k * width : (k + 1) * width] = part.astype(BF16)
    both[:, 2 * width :] = jnp.broadcast_to(squares, (batch, LANES))
    sent[:, 2 * width :] = high_and_low(squares, batch)


def high_and_low(squares, batch):
    high = squares.astype(BF16).astype(F32)
    low = lane_of((batch, LANES)) >= LANES // 2
    return jnp.where(low, squares - high, high).astype(BF16)


def gathered_sums(own, others):
    width = own.shape[1] - LANES
    sums = own[:, :width]
    squares = own[:, width : width + 1]
    for p in others:
        sums = sums + p[:, :width].astype(F32)
        tail = p[:, width:].astype(F32)
        squares = squares + (tail[:, :1] + tail[:, LANES // 2 : LANES // 2 + 1])
    return sums, squares


def middle_body(own, a, b, c, both, sent):
    sums, squares = gathered_sums(own, (a, b, c))
    batch, width = sums.shape
    both[:, :width] = sums
    sent[:, :width] = sums.astype(BF16)
    both[:, width:] = jnp.broadcast_to(squares, (batch, LANES))
    sent[:, width:] = high_and_low(squares, batch)


def down_body(own, a, b, c, weight, out):
    sums, squares = gathered_sums(own, (a, b, c))
    width = sums.shape[1] // 2
    inv = lax.rsqrt(squares / D + eps)
    gate, up = sums[:, :width] * inv, sums[:, width:] * inv
    hidden = (gate / (1.0 + jnp.exp(-gate)) * up).astype(BF16)
    out[...] = jnp.dot(hidden, weight[...], preferred_element_type=F32).astype(BF16)


def per_device(
    hidden_in,
    attn_gain,
    query_weight,
    key_cache,
    value_cache,
    lambdas,
    head_gain,
    out_weight,
    mixer_gain,
    gate_weight,
    up_weight,
    down_weight,
):
    batch, cols = hidden_in.shape
    width_q = query_weight.shape[1]
    heads = width_q // LANES
    wide = query_weight.shape[0]
    positions = key_cache.shape[1]
    shape = jax.ShapeDtypeStruct
    core = lax.axis_index(TP[1])
    chip = lax.axis_index(TP[0]).astype(jnp.int32)

    own = pl.pallas_call(
        pack_body,
        out_shape=shape((batch + 8, LANES), F32),
        in_specs=[pl.BlockSpec(memory_space=pltpu.HBM)] * 2,
        out_specs=pl.BlockSpec(memory_space=pltpu.VMEM),
        scratch_shapes=[
            pltpu.VMEM((batch, cols), BF16),
            pltpu.VMEM((1, cols), F32),
            pltpu.SemaphoreType.DMA((2,)),
        ],
        compiler_params=pltpu.CompilerParams(vmem_limit_bytes=4 * 2**20),
        cost_estimate=pl.CostEstimate(flops=COST, bytes_accessed=COST, transcendentals=0),
    )(
        pltpu.with_memory_space_constraint(hidden_in, pltpu.HBM),
        pltpu.with_memory_space_constraint(mixer_gain[None], pltpu.HBM),
    )
    mine = lane_of(own.shape) // cols % 2 == core
    pair = jnp.where(mine, own, partner(own))
    packed, block = kernel_call(
        query_body,
        [shape((batch, width_q + LANES), F32), shape((own.shape[0], wide), F32)],
        [pltpu.VMEM((4, *own.shape), F32)],
        smem=1,
        n_in=7,
        cost=COST,
    )(chip[None], pair, *peers(pair, "tp_0", "rows"), attn_gain[None], query_weight)
    packed = added(partner(packed), peers(packed, "kv_1", "query"))
    state = kernel_call(
        attend_body,
        [shape(((batch + 1) * 2 * heads, LANES), F32)],
        [
            pltpu.VMEM((heads * batch, LANES), F32),
            pltpu.VMEM((2 * heads * batch, positions), F32),
            pltpu.VMEM((batch, 2 * heads, positions), BF16),
        ],
        n_in=6,
    )(
        partner(packed),
        *peers(packed, "kv_0", "query"),
        key_cache.reshape(batch, positions, LANES),
        value_cache.reshape(batch, positions, LANES),
    )[0]
    state = kernel_call(merge_body, [shape(state.shape, F32)], n_in=4)(
        state, *peers(state, "kv_1", "heads")
    )[0]
    projected = kernel_call(
        project_body,
        [shape((batch, wide), BF16)],
        [pltpu.VMEM((2 * heads * batch, LANES), F32)],
        n_in=7,
    )(
        lambdas[None],
        state,
        *peers(state, "kv_0", "heads"),
        head_gain[None],
        out_weight,
    )[0]
    attn = added(
        projected.astype(F32), [p.astype(F32) for p in peers(projected, "tp_0", "attn")]
    )
    width = gate_weight.shape[1]
    both_shape = (batch, 2 * width + LANES)
    both, sent, after = kernel_call(
        gate_body,
        [shape(both_shape, F32), shape(both_shape, BF16), shape((batch, wide), F32)],
        n_in=5,
    )(attn, partner(attn), block, gate_weight, up_weight)
    both, sent = kernel_call(
        middle_body, [shape(both_shape, F32), shape(both_shape, BF16)], n_in=4
    )(both, *peers(sent, "kv_1", "gates"))
    down = kernel_call(down_body, [shape((batch, wide), BF16)], n_in=5)(
        both, *peers(sent, "kv_0", "gates"), down_weight
    )[0]
    mix = added(down.astype(F32), [p.astype(F32) for p in peers(down, "tp_0", "mix")])
    mixed = after + (mix + partner(mix))
    return lax.dynamic_slice_in_dim(mixed, (chip * 2 + core) * cols, cols, 1).astype(BF16)


def solution(mesh):
    split = Mesh(mesh.devices.reshape(4, 4, 4, 2), ("kv_0", "kv_1", "tp_0", "tp_1"))
    placed = (
        P(None, KV_TP),
        P(KV),
        P(KV, TP),
        P(None, KV, TP, None),
        P(None, KV, TP, None),
        P(TP),
        P(),
        P(TP, KV),
        P(KV_TP),
        P(KV, TP),
        P(KV, TP),
        P(TP, KV),
    )
    return jax.shard_map(
        per_device, mesh=split, in_specs=placed, out_specs=P(None, KV_TP), check_vma=False
    )
```

```python
import functools

import jax
import jax.numpy as jnp
from jax import lax
from jax.experimental import pallas as pl
from jax.experimental.pallas import tpu as pltpu
from jax.sharding import Mesh
from jax.sharding import PartitionSpec as P


D = 4096
HEAD_DIM = 64
KV = ("kv_0", "kv_1")
KV_TP = ("kv_0", "kv_1", "tp_0", "tp_1")
TP = ("tp_0", "tp_1")
LANES = 128
F32 = jnp.float32
BF16 = jnp.bfloat16

eps = 1e-06
COST = 2**40

SHIFTS = (2, 3, 1)
STRAIGHT = ("gates",)


def peers(shard, axis, what):
    across, wide = (axis, 1) if what in STRAIGHT else ((axis, TP[1]), 2)
    n = lax.axis_size(across)
    got = []
    for s in SHIFTS:
        pairs = [(i, i ^ (wide * s + wide - 1)) for i in range(n)]
        got.append(lax.ppermute(shard, across, pairs))
    return got


def partner(shard):
    return lax.ppermute(shard, TP[1], [(0, 1), (1, 0)])


def added(own, got):
    for p in got:
        own = own + p
    return own


def lane_of(shape):
    return lax.broadcasted_iota(jnp.int32, shape, len(shape) - 1)


def kernel_call(body, outs, scratch=(), smem=0, n_in=1, mib=16, cost=0):
    spec = [pl.BlockSpec(memory_space=pltpu.SMEM)] * smem
    spec += [pl.BlockSpec(memory_space=pltpu.VMEM)] * (n_in - smem)
    return pl.pallas_call(
        body,
        out_shape=outs,
        in_specs=spec,
        out_specs=[pl.BlockSpec(memory_space=pltpu.VMEM)] * len(outs),
        scratch_shapes=scratch,
        compiler_params=pltpu.CompilerParams(vmem_limit_bytes=mib * 2**20),
        cost_estimate=pl.CostEstimate(flops=cost, bytes_accessed=cost, transcendentals=0)
        if cost
        else None,
    )


def pack_body(hidden, gain, out, rows, scale, sems):
    loads = [
        pltpu.make_async_copy(hidden, rows, sems.at[0]),
        pltpu.make_async_copy(gain, scale, sems.at[1]),
    ]
    for load in loads:
        load.start()
    for load in loads:
        load.wait()
    batch, cols = hidden.shape
    out[:batch, :] = jnp.concatenate([rows[...].astype(F32)] * (LANES // cols), axis=1)
    row = jnp.concatenate([scale[...]] * (LANES // cols), axis=1)
    out[batch:, :] = jnp.broadcast_to(row, (out.shape[0] - batch, LANES))


def query_body(chip, own, a, b, c, gain, weight, packed, block, held):
    batch = packed.shape[0]
    x = chip[0]
    held[x] = own[...]
    for s, ref in zip(SHIFTS, (a, b, c)):
        held[x ^ s] = ref[...]
    left = lane_of(own.shape) < LANES // 2
    for t in range(2):
        block[:, t * LANES : (t + 1) * LANES] = jnp.where(left, held[2 * t], held[2 * t + 1])
    rows = block[:batch, :]
    gained = (rows * gain[...]).astype(BF16)
    width = weight.shape[1]
    packed[:, :width] = jnp.dot(gained, weight[...], preferred_element_type=F32)
    squares = jnp.sum(rows * rows, axis=1, keepdims=True)
    packed[:, width:] = jnp.broadcast_to(squares, (batch, LANES))


def attend_body(own, a, b, c, keys, values, out, sent, query, scores, weights):
    batch, _, _ = keys.shape
    width = own.shape[1] - LANES
    heads = width // LANES
    whole = own[...] + a[...] + b[...] + c[...]
    inv = lax.rsqrt(whole[:, width:] / D + eps)
    for g in range(heads):
        part = whole[:, g * LANES : (g + 1) * LANES] * inv
        query[g * batch : (g + 1) * batch, :] = part.astype(BF16).astype(F32)
    shape = (2 * heads, LANES)
    half = lane_of(shape) // HEAD_DIM
    keep = half == lax.broadcasted_iota(jnp.int32, shape, 0) // heads
    lane = lane_of(shape)
    high = 2 * heads
    for n in range(batch):
        q = query[pl.ds(n, heads, stride=batch), :]
        q = jnp.where(keep, jnp.concatenate([q, q], axis=0), 0.0).astype(BF16)
        scores[n * high : (n + 1) * high, :] = lax.dot_general(
            q, keys[n], (((1,), (1,)), ((), ())), preferred_element_type=F32
        )
    stats = jnp.zeros(shape, F32)
    for n in range(batch):
        score = scores[n * high : (n + 1) * high, :] * HEAD_DIM ** (-0.5)
        top = jnp.max(score, axis=1, keepdims=True)
        exponent = jnp.exp(score - top)
        total = jnp.sum(exponent, axis=1, keepdims=True)
        weights[n] = exponent.astype(BF16)
        stats = jnp.where(lane == n, top, stats)
        stats = jnp.where(lane == n + LANES // 2, total, stats)
    out[batch * high :, :] = stats
    for n in range(batch):
        out[n * high : (n + 1) * high, :] = jnp.dot(
            weights[n], values[n], preferred_element_type=F32
        )
    write_sent(sent, out[: batch * high, :], stats)


def three_parts(stats):
    high = stats.astype(BF16).astype(F32)
    rest = stats - high
    middle = rest.astype(BF16).astype(F32)
    low = rest - middle
    return high + pltpu.roll(middle, 16, 1) + pltpu.roll(low, 32, 1)


def from_parts(parts):
    whole = (parts + pltpu.roll(parts, LANES - 16, 1)) + pltpu.roll(parts, LANES - 32, 1)
    return jnp.where(lane_of(parts.shape) % (LANES // 2) < 16, whole, 0.0)


def write_sent(sent, accs, stats):
    n = accs.shape[0]
    sent[:n, :] = accs.astype(BF16)
    sent[n:, :] = jnp.concatenate([three_parts(stats)] * 2, axis=0).astype(BF16)


def combined(own, others, high):
    n = own.shape[0] - high
    stats = [own[n:, :]] + [from_parts(p[n:, :].astype(F32)[:high]) for p in others]
    values = [own[:n, :]] + [p[:n, :].astype(F32) for p in others]
    top = functools.reduce(jnp.maximum, stats)
    factors = [jnp.exp(s - top) for s in stats]
    shifted = [pltpu.roll(f, LANES // 2, 1) for f in factors]
    total = sum(s * f for s, f in zip(stats, shifted))
    low = lane_of(top.shape) < LANES // 2
    accs = []
    for k in range(n // high):
        acc = 0.0
        for v, f in zip(values, factors):
            acc = acc + v[k * high : (k + 1) * high] * f[:, k : k + 1]
        accs.append(acc)
    return jnp.where(low, top, total), accs


def merge_body(own, a, b, c, out, sent):
    stats, accs = combined(own, (a, b, c), 8)
    accs = jnp.concatenate(accs, axis=0)
    out[: accs.shape[0], :] = accs
    out[accs.shape[0] :, :] = stats
    write_sent(sent, accs, stats)


def project_body(lambdas, own, a, b, c, gain, weight, out, held):
    high = 8
    heads = high // 2
    rows = own.shape[0] // high - 1
    stats, accs = combined(own, (a, b, c), high)
    inverse = 1.0 / stats
    for k, acc in enumerate(accs):
        at_lane = LANES // 2 + k
        held[k * high : (k + 1) * high, :] = acc * inverse[:, at_lane : at_lane + 1]
    projected = 0.0
    for g in range(heads):
        first = held[pl.ds(g, rows, stride=high), :]
        second = held[pl.ds(heads + g, rows, stride=high), :]
        attended = first - lambdas[:, g : g + 1] * second
        norm = lax.rsqrt(jnp.mean(attended * attended, axis=1, keepdims=True) + eps)
        projected = projected + jnp.dot(
            (attended * norm * gain[...]).astype(BF16),
            weight[g * LANES : (g + 1) * LANES, :],
            preferred_element_type=F32,
        )
    out[...] = projected.astype(BF16)


def gate_body(attn, other, block, gate, up, both, sent, after):
    batch = attn.shape[0]
    rows = (block[:batch, :] + (attn[...] + other[...])).astype(BF16).astype(F32)
    after[...] = rows
    squares = jnp.sum(rows * rows, axis=1, keepdims=True)
    mixer_in = (rows * block[batch : batch + 1, :]).astype(BF16)
    width = gate.shape[1]
    for k, weight in enumerate((gate, up)):
        part = jnp.dot(mixer_in, weight[...], preferred_element_type=F32)
        both[:, k * width : (k + 1) * width] = part
        sent[:, k * width : (k + 1) * width] = part.astype(BF16)
    both[:, 2 * width :] = jnp.broadcast_to(squares, (batch, LANES))
    sent[:, 2 * width :] = high_and_low(squares, batch)


def high_and_low(squares, batch):
    high = squares.astype(BF16).astype(F32)
    low = lane_of((batch, LANES)) >= LANES // 2
    return jnp.where(low, squares - high, high).astype(BF16)


def gathered_sums(own, others):
    width = own.shape[1] - LANES
    sums = own[:, :width]
    squares = own[:, width : width + 1]
    for p in others:
        sums = sums + p[:, :width].astype(F32)
        tail = p[:, width:].astype(F32)
        squares = squares + (tail[:, :1] + tail[:, LANES // 2 : LANES // 2 + 1])
    return sums, squares


def middle_body(own, a, b, c, both, sent):
    sums, squares = gathered_sums(own, (a, b, c))
    batch, width = sums.shape
    both[:, :width] = sums
    sent[:, :width] = sums.astype(BF16)
    both[:, width:] = jnp.broadcast_to(squares, (batch, LANES))
    sent[:, width:] = high_and_low(squares, batch)


def down_body(own, a, b, c, weight, out):
    sums, squares = gathered_sums(own, (a, b, c))
    width = sums.shape[1] // 2
    inv = lax.rsqrt(squares / D + eps)
    gate, up = sums[:, :width] * inv, sums[:, width:] * inv
    hidden = (gate / (1.0 + jnp.exp(-gate)) * up).astype(BF16)
    out[...] = jnp.dot(hidden, weight[...], preferred_element_type=F32).astype(BF16)


def per_device(
    hidden_in,
    attn_gain,
    query_weight,
    key_cache,
    value_cache,
    lambdas,
    head_gain,
    out_weight,
    mixer_gain,
    gate_weight,
    up_weight,
    down_weight,
):
    batch, cols = hidden_in.shape
    width_q = query_weight.shape[1]
    heads = width_q // LANES
    wide = query_weight.shape[0]
    positions = key_cache.shape[1]
    shape = jax.ShapeDtypeStruct
    core = lax.axis_index(TP[1])
    chip = lax.axis_index(TP[0]).astype(jnp.int32)

    own = pl.pallas_call(
        pack_body,
        out_shape=shape((batch + 8, LANES), F32),
        in_specs=[pl.BlockSpec(memory_space=pltpu.HBM)] * 2,
        out_specs=pl.BlockSpec(memory_space=pltpu.VMEM),
        scratch_shapes=[
            pltpu.VMEM((batch, cols), BF16),
            pltpu.VMEM((1, cols), F32),
            pltpu.SemaphoreType.DMA((2,)),
        ],
        compiler_params=pltpu.CompilerParams(vmem_limit_bytes=4 * 2**20),
        cost_estimate=pl.CostEstimate(flops=COST, bytes_accessed=COST, transcendentals=0),
    )(
        pltpu.with_memory_space_constraint(hidden_in, pltpu.HBM),
        pltpu.with_memory_space_constraint(mixer_gain[None], pltpu.HBM),
    )
    mine = lane_of(own.shape) // cols % 2 == core
    pair = jnp.where(mine, own, partner(own))
    packed, block = kernel_call(
        query_body,
        [shape((batch, width_q + LANES), F32), shape((own.shape[0], wide), F32)],
        [pltpu.VMEM((4, *own.shape), F32)],
        smem=1,
        n_in=7,
        cost=COST,
    )(chip[None], pair, *peers(pair, "tp_0", "rows"), attn_gain[None], query_weight)
    packed = added(partner(packed), peers(packed, "kv_1", "query"))
    rows = batch * 2 * heads
    states = [shape((rows + 8, LANES), F32), shape((rows + 16, LANES), BF16)]
    state, sent = kernel_call(
        attend_body,
        states,
        [
            pltpu.VMEM((heads * batch, LANES), F32),
            pltpu.VMEM((2 * heads * batch, positions), F32),
            pltpu.VMEM((batch, 2 * heads, positions), BF16),
        ],
        n_in=6,
    )(
        partner(packed),
        *peers(packed, "kv_0", "query"),
        key_cache.reshape(batch, positions, LANES),
        value_cache.reshape(batch, positions, LANES),
    )
    state, sent = kernel_call(merge_body, states, n_in=4)(
        partner(state), *peers(sent, "kv_1", "heads")
    )
    projected = kernel_call(
        project_body,
        [shape((batch, wide), BF16)],
        [pltpu.VMEM((2 * heads * batch, LANES), F32)],
        n_in=7,
    )(lambdas[None], partner(state), *peers(sent, "kv_0", "heads"), head_gain[None], out_weight)[0]
    attn = added(
        projected.astype(F32), [p.astype(F32) for p in peers(projected, "tp_0", "attn")]
    )
    width = gate_weight.shape[1]
    both_shape = (batch, 2 * width + LANES)
    both, sent, after = kernel_call(
        gate_body,
        [shape(both_shape, F32), shape(both_shape, BF16), shape((batch, wide), F32)],
        n_in=5,
    )(attn, partner(attn), block, gate_weight, up_weight)
    both, sent = kernel_call(
        middle_body, [shape(both_shape, F32), shape(both_shape, BF16)], n_in=4
    )(both, *peers(sent, "kv_1", "gates"))
    down = kernel_call(down_body, [shape((batch, wide), BF16)], n_in=5)(
        both, *peers(sent, "kv_0", "gates"), down_weight
    )[0]
    mix = added(down.astype(F32), [p.astype(F32) for p in peers(down, "tp_0", "mix")])
    mixed = after + (mix + partner(mix))
    return lax.dynamic_slice_in_dim(mixed, (chip * 2 + core) * cols, cols, 1).astype(BF16)


def solution(mesh):
    split = Mesh(mesh.devices.reshape(4, 4, 4, 2), ("kv_0", "kv_1", "tp_0", "tp_1"))
    placed = (
        P(None, KV_TP),
        P(KV),
        P(KV, TP),
        P(None, KV, TP, None),
        P(None, KV, TP, None),
        P(TP),
        P(),
        P(TP, KV),
        P(KV_TP),
        P(KV, TP),
        P(KV, TP),
        P(TP, KV),
    )
    return jax.shard_map(
        per_device, mesh=split, in_specs=placed, out_specs=P(None, KV_TP), check_vma=False
    )
```

```python
import functools

import jax
import jax.numpy as jnp
from jax import lax
from jax.experimental import pallas as pl
from jax.experimental.pallas import tpu as pltpu
from jax.sharding import Mesh
from jax.sharding import PartitionSpec as P


D = 4096
HEAD_DIM = 64
KV = ("kv_0", "kv_1")
KV_TP = ("kv_0", "kv_1", "tp_0", "tp_1")
TP = ("tp_0", "tp_1")
LANES = 128
F32 = jnp.float32
BF16 = jnp.bfloat16

eps = 1e-06
COST = 2**40

SHIFTS = (2, 3, 1)
STRAIGHT = ("gates",)


def peers(shard, axis, what):
    if what in STRAIGHT:
        return kv_peers(shard, axis, what)
    across, wide = (axis, 1) if what in STRAIGHT else ((axis, TP[1]), 2)
    n = lax.axis_size(across)
    got = []
    for s in SHIFTS:
        pairs = [(i, i ^ (wide * s + wide - 1)) for i in range(n)]
        got.append(lax.ppermute(shard, across, pairs))
    return got


def kv_peers(shard, axis, what):
    n = lax.axis_size(KV[0])
    got = []
    for s in SHIFTS:
        pairs = []
        for z in range(n):
            for y in range(n):
                for c in range(2):
                    straight = what in STRAIGHT
                    inner = c == 0 if not straight or axis == KV[1] else c == 1
                    to_z, to_y = (z, y ^ s) if inner else (z ^ s, y)
                    to_c = c if straight else 1 - c
                    pairs.append(((z * n + y) * 2 + c, (to_z * n + to_y) * 2 + to_c))
        got.append(lax.ppermute(shard, (*KV, TP[1]), pairs))
    return got


def partner(shard):
    return lax.ppermute(shard, TP[1], [(0, 1), (1, 0)])


def added(own, got):
    for p in got:
        own = own + p
    return own


def lane_of(shape):
    return lax.broadcasted_iota(jnp.int32, shape, len(shape) - 1)


def kernel_call(body, outs, scratch=(), smem=0, n_in=1, mib=16, cost=0):
    spec = [pl.BlockSpec(memory_space=pltpu.SMEM)] * smem
    spec += [pl.BlockSpec(memory_space=pltpu.VMEM)] * (n_in - smem)
    return pl.pallas_call(
        body,
        out_shape=outs,
        in_specs=spec,
        out_specs=[pl.BlockSpec(memory_space=pltpu.VMEM)] * len(outs),
        scratch_shapes=scratch,
        compiler_params=pltpu.CompilerParams(vmem_limit_bytes=mib * 2**20),
        cost_estimate=pl.CostEstimate(flops=cost, bytes_accessed=cost, transcendentals=0)
        if cost
        else None,
    )


def pack_body(hidden, gain, out, rows, scale, sems):
    loads = [
        pltpu.make_async_copy(hidden, rows, sems.at[0]),
        pltpu.make_async_copy(gain, scale, sems.at[1]),
    ]
    for load in loads:
        load.start()
    for load in loads:
        load.wait()
    batch, cols = hidden.shape
    out[:batch, :] = jnp.concatenate([rows[...].astype(F32)] * (LANES // cols), axis=1)
    row = jnp.concatenate([scale[...]] * (LANES // cols), axis=1)
    out[batch:, :] = jnp.broadcast_to(row, (out.shape[0] - batch, LANES))


def query_body(chip, own, a, b, c, gain, weight, packed, block, held):
    batch = packed.shape[0]
    x = chip[0]
    held[x] = own[...]
    for s, ref in zip(SHIFTS, (a, b, c)):
        held[x ^ s] = ref[...]
    left = lane_of(own.shape) < LANES // 2
    for t in range(2):
        block[:, t * LANES : (t + 1) * LANES] = jnp.where(left, held[2 * t], held[2 * t + 1])
    rows = block[:batch, :]
    gained = (rows * gain[...]).astype(BF16)
    width = weight.shape[1]
    packed[:, :width] = jnp.dot(gained, weight[...], preferred_element_type=F32)
    squares = jnp.sum(rows * rows, axis=1, keepdims=True)
    packed[:, width:] = jnp.broadcast_to(squares, (batch, LANES))


def attend_body(own, a, b, c, keys, values, out, sent, query, scores, weights):
    batch, _, _ = keys.shape
    width = own.shape[1] - LANES
    heads = width // LANES
    whole = own[...] + a[...] + b[...] + c[...]
    inv = lax.rsqrt(whole[:, width:] / D + eps)
    for g in range(heads):
        part = whole[:, g * LANES : (g + 1) * LANES] * inv
        query[g * batch : (g + 1) * batch, :] = part.astype(BF16).astype(F32)
    shape = (2 * heads, LANES)
    half = lane_of(shape) // HEAD_DIM
    keep = half == lax.broadcasted_iota(jnp.int32, shape, 0) // heads
    lane = lane_of(shape)
    high = 2 * heads
    for n in range(batch):
        q = query[pl.ds(n, heads, stride=batch), :]
        q = jnp.where(keep, jnp.concatenate([q, q], axis=0), 0.0).astype(BF16)
        scores[n * high : (n + 1) * high, :] = lax.dot_general(
            q, keys[n], (((1,), (1,)), ((), ())), preferred_element_type=F32
        )
    stats = jnp.zeros(shape, F32)
    for n in range(batch):
        score = scores[n * high : (n + 1) * high, :] * HEAD_DIM ** (-0.5)
        top = jnp.max(score, axis=1, keepdims=True)
        exponent = jnp.exp(score - top)
        total = jnp.sum(exponent, axis=1, keepdims=True)
        weights[n] = exponent.astype(BF16)
        stats = jnp.where(lane == n, top, stats)
        stats = jnp.where(lane == n + LANES // 2, total, stats)
    out[batch * high :, :] = stats
    for n in range(batch):
        out[n * high : (n + 1) * high, :] = jnp.dot(
            weights[n], values[n], preferred_element_type=F32
        )
    write_sent(sent, out[: batch * high, :], stats)


def three_parts(stats):
    high = stats.astype(BF16).astype(F32)
    rest = stats - high
    middle = rest.astype(BF16).astype(F32)
    low = rest - middle
    return high + pltpu.roll(middle, 16, 1) + pltpu.roll(low, 32, 1)


def from_parts(parts):
    whole = (parts + pltpu.roll(parts, LANES - 16, 1)) + pltpu.roll(parts, LANES - 32, 1)
    return jnp.where(lane_of(parts.shape) % (LANES // 2) < 16, whole, 0.0)


def write_sent(sent, accs, stats):
    n = accs.shape[0]
    sent[:n, :] = accs.astype(BF16)
    sent[n:, :] = jnp.concatenate([three_parts(stats)] * 2, axis=0).astype(BF16)


def combined(own, others, high):
    n = own.shape[0] - high
    stats = [own[n:, :]] + [from_parts(p[n:, :].astype(F32)[:high]) for p in others]
    values = [own[:n, :]] + [p[:n, :].astype(F32) for p in others]
    top = functools.reduce(jnp.maximum, stats)
    factors = [jnp.exp(s - top) for s in stats]
    shifted = [pltpu.roll(f, LANES // 2, 1) for f in factors]
    total = sum(s * f for s, f in zip(stats, shifted))
    low = lane_of(top.shape) < LANES // 2
    accs = []
    for k in range(n // high):
        acc = 0.0
        for v, f in zip(values, factors):
            acc = acc + v[k * high : (k + 1) * high] * f[:, k : k + 1]
        accs.append(acc)
    return jnp.where(low, top, total), accs


def merge_body(own, a, b, c, out, sent):
    stats, accs = combined(own, (a, b, c), 8)
    accs = jnp.concatenate(accs, axis=0)
    out[: accs.shape[0], :] = accs
    out[accs.shape[0] :, :] = stats
    write_sent(sent, accs, stats)


def project_body(lambdas, own, a, b, c, gain, weight, out, held):
    high = 8
    heads = high // 2
    rows = own.shape[0] // high - 1
    stats, accs = combined(own, (a, b, c), high)
    inverse = 1.0 / stats
    for k, acc in enumerate(accs):
        at_lane = LANES // 2 + k
        held[k * high : (k + 1) * high, :] = acc * inverse[:, at_lane : at_lane + 1]
    projected = 0.0
    for g in range(heads):
        first = held[pl.ds(g, rows, stride=high), :]
        second = held[pl.ds(heads + g, rows, stride=high), :]
        attended = first - lambdas[:, g : g + 1] * second
        norm = lax.rsqrt(jnp.mean(attended * attended, axis=1, keepdims=True) + eps)
        projected = projected + jnp.dot(
            (attended * norm * gain[...]).astype(BF16),
            weight[g * LANES : (g + 1) * LANES, :],
            preferred_element_type=F32,
        )
    out[...] = projected.astype(BF16)


def gate_body(attn, other, block, gate, up, both, sent, after):
    batch = attn.shape[0]
    rows = (block[:batch, :] + (attn[...] + other[...])).astype(BF16).astype(F32)
    after[...] = rows
    squares = jnp.sum(rows * rows, axis=1, keepdims=True)
    mixer_in = (rows * block[batch : batch + 1, :]).astype(BF16)
    width = gate.shape[1]
    for k, weight in enumerate((gate, up)):
        part = jnp.dot(mixer_in, weight[...], preferred_element_type=F32)
        both[:, k * width : (k + 1) * width] = part
        sent[:, k * width : (k + 1) * width] = part.astype(BF16)
    both[:, 2 * width :] = jnp.broadcast_to(squares, (batch, LANES))
    sent[:, 2 * width :] = high_and_low(squares, batch)


def high_and_low(squares, batch):
    high = squares.astype(BF16).astype(F32)
    low = lane_of((batch, LANES)) >= LANES // 2
    return jnp.where(low, squares - high, high).astype(BF16)


def gathered_sums(own, others):
    width = own.shape[1] - LANES
    sums = own[:, :width]
    squares = own[:, width : width + 1]
    for p in others:
        sums = sums + p[:, :width].astype(F32)
        tail = p[:, width:].astype(F32)
        squares = squares + (tail[:, :1] + tail[:, LANES // 2 : LANES // 2 + 1])
    return sums, squares


def middle_body(own, a, b, c, both, sent):
    sums, squares = gathered_sums(own, (a, b, c))
    batch, width = sums.shape
    both[:, :width] = sums
    sent[:, :width] = sums.astype(BF16)
    both[:, width:] = jnp.broadcast_to(squares, (batch, LANES))
    sent[:, width:] = high_and_low(squares, batch)


def down_body(own, a, b, c, weight, out):
    sums, squares = gathered_sums(own, (a, b, c))
    width = sums.shape[1] // 2
    inv = lax.rsqrt(squares / D + eps)
    gate, up = sums[:, :width] * inv, sums[:, width:] * inv
    hidden = (gate / (1.0 + jnp.exp(-gate)) * up).astype(BF16)
    out[...] = jnp.dot(hidden, weight[...], preferred_element_type=F32).astype(BF16)


def per_device(
    hidden_in,
    attn_gain,
    query_weight,
    key_cache,
    value_cache,
    lambdas,
    head_gain,
    out_weight,
    mixer_gain,
    gate_weight,
    up_weight,
    down_weight,
):
    batch, cols = hidden_in.shape
    width_q = query_weight.shape[1]
    heads = width_q // LANES
    wide = query_weight.shape[0]
    positions = key_cache.shape[1]
    shape = jax.ShapeDtypeStruct
    core = lax.axis_index(TP[1])
    chip = lax.axis_index(TP[0]).astype(jnp.int32)

    own = pl.pallas_call(
        pack_body,
        out_shape=shape((batch + 8, LANES), F32),
        in_specs=[pl.BlockSpec(memory_space=pltpu.HBM)] * 2,
        out_specs=pl.BlockSpec(memory_space=pltpu.VMEM),
        scratch_shapes=[
            pltpu.VMEM((batch, cols), BF16),
            pltpu.VMEM((1, cols), F32),
            pltpu.SemaphoreType.DMA((2,)),
        ],
        compiler_params=pltpu.CompilerParams(vmem_limit_bytes=4 * 2**20),
        cost_estimate=pl.CostEstimate(flops=COST, bytes_accessed=COST, transcendentals=0),
    )(
        pltpu.with_memory_space_constraint(hidden_in, pltpu.HBM),
        pltpu.with_memory_space_constraint(mixer_gain[None], pltpu.HBM),
    )
    mine = lane_of(own.shape) // cols % 2 == core
    pair = jnp.where(mine, own, partner(own))
    packed, block = kernel_call(
        query_body,
        [shape((batch, width_q + LANES), F32), shape((own.shape[0], wide), F32)],
        [pltpu.VMEM((4, *own.shape), F32)],
        smem=1,
        n_in=7,
        cost=COST,
    )(chip[None], pair, *peers(pair, "tp_0", "rows"), attn_gain[None], query_weight)
    packed = added(partner(packed), peers(packed, "kv_1", "query"))
    rows = batch * 2 * heads
    states = [shape((rows + 8, LANES), F32), shape((rows + 16, LANES), BF16)]
    state, sent = kernel_call(
        attend_body,
        states,
        [
            pltpu.VMEM((heads * batch, LANES), F32),
            pltpu.VMEM((2 * heads * batch, positions), F32),
            pltpu.VMEM((batch, 2 * heads, positions), BF16),
        ],
        n_in=6,
    )(
        partner(packed),
        *peers(packed, "kv_0", "query"),
        key_cache.reshape(batch, positions, LANES),
        value_cache.reshape(batch, positions, LANES),
    )
    state, sent = kernel_call(merge_body, states, n_in=4)(
        partner(state), *peers(sent, "kv_1", "heads")
    )
    projected = kernel_call(
        project_body,
        [shape((batch, wide), BF16)],
        [pltpu.VMEM((2 * heads * batch, LANES), F32)],
        n_in=7,
    )(lambdas[None], partner(state), *peers(sent, "kv_0", "heads"), head_gain[None], out_weight)[0]
    attn = added(
        projected.astype(F32), [p.astype(F32) for p in peers(projected, "tp_0", "attn")]
    )
    width = gate_weight.shape[1]
    both_shape = (batch, 2 * width + LANES)
    both, sent, after = kernel_call(
        gate_body,
        [shape(both_shape, F32), shape(both_shape, BF16), shape((batch, wide), F32)],
        n_in=5,
    )(attn, partner(attn), block, gate_weight, up_weight)
    both, sent = kernel_call(
        middle_body, [shape(both_shape, F32), shape(both_shape, BF16)], n_in=4
    )(both, *peers(sent, "kv_1", "gates"))
    down = kernel_call(down_body, [shape((batch, wide), BF16)], n_in=5)(
        both, *peers(sent, "kv_0", "gates"), down_weight
    )[0]
    mix = added(down.astype(F32), [p.astype(F32) for p in peers(down, "tp_0", "mix")])
    mixed = after + (mix + partner(mix))
    return lax.dynamic_slice_in_dim(mixed, (chip * 2 + core) * cols, cols, 1).astype(BF16)


def solution(mesh):
    split = Mesh(mesh.devices.reshape(4, 4, 4, 2), ("kv_0", "kv_1", "tp_0", "tp_1"))
    placed = (
        P(None, KV_TP),
        P(KV),
        P(KV, TP),
        P(None, KV, TP, None),
        P(None, KV, TP, None),
        P(TP),
        P(),
        P(TP, KV),
        P(KV_TP),
        P(KV, TP),
        P(KV, TP),
        P(TP, KV),
    )
    return jax.shard_map(
        per_device, mesh=split, in_specs=placed, out_specs=P(None, KV_TP), check_vma=False
    )
```

```python
import functools

import jax
import jax.numpy as jnp
from jax import lax
from jax.experimental import pallas as pl
from jax.experimental.pallas import tpu as pltpu
from jax.sharding import Mesh
from jax.sharding import PartitionSpec as P


D = 4096
HEAD_DIM = 64
KV = ("kv_0", "kv_1")
KV_TP = ("kv_0", "kv_1", "tp_0", "tp_1")
TP = ("tp_0", "tp_1")
LANES = 128
F32 = jnp.float32
BF16 = jnp.bfloat16

eps = 1e-06
COST = 2**40

SHIFTS = (2, 3, 1)
STRAIGHT = ("gates",)


def peers(shard, axis, what):
    if what in STRAIGHT:
        return kv_peers(shard, axis, what)
    across, wide = (axis, 1) if what in STRAIGHT else ((axis, TP[1]), 2)
    n = lax.axis_size(across)
    got = []
    for s in SHIFTS:
        pairs = [(i, i ^ (wide * s + wide - 1)) for i in range(n)]
        got.append(lax.ppermute(shard, across, pairs))
    return got


def kv_peers(shard, axis, what):
    n = lax.axis_size(KV[0])
    got = []
    for s in SHIFTS:
        pairs = []
        for z in range(n):
            for y in range(n):
                for c in range(2):
                    straight = what in STRAIGHT
                    inner = c == 0 if not straight or axis == KV[1] else c == 1
                    to_z, to_y = (z, y ^ s) if inner else (z ^ s, y)
                    to_c = c if straight else 1 - c
                    pairs.append(((z * n + y) * 2 + c, (to_z * n + to_y) * 2 + to_c))
        got.append(lax.ppermute(shard, (*KV, TP[1]), pairs))
    return got


def partner(shard):
    return lax.ppermute(shard, TP[1], [(0, 1), (1, 0)])


def added(own, got):
    for p in got:
        own = own + p
    return own


def lane_of(shape):
    return lax.broadcasted_iota(jnp.int32, shape, len(shape) - 1)


def kernel_call(body, outs, scratch=(), smem=0, n_in=1, mib=16, cost=0):
    spec = [pl.BlockSpec(memory_space=pltpu.SMEM)] * smem
    spec += [pl.BlockSpec(memory_space=pltpu.VMEM)] * (n_in - smem)
    return pl.pallas_call(
        body,
        out_shape=outs,
        in_specs=spec,
        out_specs=[pl.BlockSpec(memory_space=pltpu.VMEM)] * len(outs),
        scratch_shapes=scratch,
        compiler_params=pltpu.CompilerParams(vmem_limit_bytes=mib * 2**20),
        cost_estimate=pl.CostEstimate(flops=cost, bytes_accessed=cost, transcendentals=0)
        if cost
        else None,
    )


def pack_body(hidden, gain, out, rows, scale, sems):
    loads = [
        pltpu.make_async_copy(hidden, rows, sems.at[0]),
        pltpu.make_async_copy(gain, scale, sems.at[1]),
    ]
    for load in loads:
        load.start()
    for load in loads:
        load.wait()
    batch, cols = hidden.shape
    out[:batch, :] = jnp.concatenate([rows[...].astype(F32)] * (LANES // cols), axis=1)
    row = jnp.concatenate([scale[...]] * (LANES // cols), axis=1)
    out[batch:, :] = jnp.broadcast_to(row, (out.shape[0] - batch, LANES))


def query_body(chip, own, a, b, c, gain, weight, packed, block, held):
    batch = own.shape[0] - 8
    x = chip[0]
    held[x] = own[...]
    for s, ref in zip(SHIFTS, (a, b, c)):
        held[x ^ s] = ref[...]
    left = lane_of(own.shape) < LANES // 2
    for t in range(2):
        block[:, t * LANES : (t + 1) * LANES] = jnp.where(left, held[2 * t], held[2 * t + 1])
    rows = block[:batch, :]
    gained = (rows * gain[...]).astype(BF16)
    width = weight.shape[1]
    product = jnp.dot(gained, weight[...], preferred_element_type=F32)
    for g in range(width // LANES):
        packed[g * batch : (g + 1) * batch, :] = product[:, g * LANES : (g + 1) * LANES]
    squares = jnp.sum(rows * rows, axis=1, keepdims=True)
    shape = (8, LANES)
    packed[width // LANES * batch :, :] = jnp.where(
        lane_of(shape) < LANES // 2,
        jnp.broadcast_to(squares[:8], shape),
        jnp.broadcast_to(squares[8:], shape),
    )


def attend_body(own, a, b, c, keys, values, out, sent, query, scores, weights):
    batch, _, _ = keys.shape
    heads = own.shape[0] // batch
    whole = own[...] + a[...] + b[...] + c[...]
    squares = whole[heads * batch :]
    squares = jnp.concatenate([squares[:, :1], squares[:, LANES // 2 : LANES // 2 + 1]], axis=0)
    inv = lax.rsqrt(squares / D + eps)
    for g in range(heads):
        part = whole[g * batch : (g + 1) * batch] * inv
        query[g * batch : (g + 1) * batch, :] = part.astype(BF16).astype(F32)
    shape = (2 * heads, LANES)
    half = lane_of(shape) // HEAD_DIM
    keep = half == lax.broadcasted_iota(jnp.int32, shape, 0) // heads
    lane = lane_of(shape)
    high = 2 * heads
    for n in range(batch):
        q = query[pl.ds(n, heads, stride=batch), :]
        q = jnp.where(keep, jnp.concatenate([q, q], axis=0), 0.0).astype(BF16)
        scores[n * high : (n + 1) * high, :] = lax.dot_general(
            q, keys[n], (((1,), (1,)), ((), ())), preferred_element_type=F32
        )
    stats = jnp.zeros(shape, F32)
    for n in range(batch):
        score = scores[n * high : (n + 1) * high, :] * HEAD_DIM ** (-0.5)
        top = jnp.max(score, axis=1, keepdims=True)
        exponent = jnp.exp(score - top)
        total = jnp.sum(exponent, axis=1, keepdims=True)
        weights[n] = exponent.astype(BF16)
        stats = jnp.where(lane == n, top, stats)
        stats = jnp.where(lane == n + LANES // 2, total, stats)
    out[batch * high :, :] = stats
    for n in range(batch):
        out[n * high : (n + 1) * high, :] = jnp.dot(
            weights[n], values[n], preferred_element_type=F32
        )
    write_sent(sent, out[: batch * high, :], stats)


def three_parts(stats):
    high = stats.astype(BF16).astype(F32)
    rest = stats - high
    middle = rest.astype(BF16).astype(F32)
    low = rest - middle
    return high + pltpu.roll(middle, 16, 1) + pltpu.roll(low, 32, 1)


def from_parts(parts):
    whole = (parts + pltpu.roll(parts, LANES - 16, 1)) + pltpu.roll(parts, LANES - 32, 1)
    return jnp.where(lane_of(parts.shape) % (LANES // 2) < 16, whole, 0.0)


def write_sent(sent, accs, stats):
    n = accs.shape[0]
    sent[:n, :] = accs.astype(BF16)
    sent[n:, :] = jnp.concatenate([three_parts(stats)] * 2, axis=0).astype(BF16)


def combined(own, others, high):
    n = own.shape[0] - high
    stats = [own[n:, :]] + [from_parts(p[n:, :].astype(F32)[:high]) for p in others]
    values = [own[:n, :]] + [p[:n, :].astype(F32) for p in others]
    top = functools.reduce(jnp.maximum, stats)
    factors = [jnp.exp(s - top) for s in stats]
    shifted = [pltpu.roll(f, LANES // 2, 1) for f in factors]
    total = sum(s * f for s, f in zip(stats, shifted))
    low = lane_of(top.shape) < LANES // 2
    accs = []
    for k in range(n // high):
        acc = 0.0
        for v, f in zip(values, factors):
            acc = acc + v[k * high : (k + 1) * high] * f[:, k : k + 1]
        accs.append(acc)
    return jnp.where(low, top, total), accs


def merge_body(own, a, b, c, out, sent):
    stats, accs = combined(own, (a, b, c), 8)
    accs = jnp.concatenate(accs, axis=0)
    out[: accs.shape[0], :] = accs
    out[accs.shape[0] :, :] = stats
    write_sent(sent, accs, stats)


def project_body(lambdas, own, a, b, c, gain, weight, out, held):
    high = 8
    heads = high // 2
    rows = own.shape[0] // high - 1
    stats, accs = combined(own, (a, b, c), high)
    inverse = 1.0 / stats
    for k, acc in enumerate(accs):
        at_lane = LANES // 2 + k
        held[k * high : (k + 1) * high, :] = acc * inverse[:, at_lane : at_lane + 1]
    projected = 0.0
    for g in range(heads):
        first = held[pl.ds(g, rows, stride=high), :]
        second = held[pl.ds(heads + g, rows, stride=high), :]
        attended = first - lambdas[:, g : g + 1] * second
        norm = lax.rsqrt(jnp.mean(attended * attended, axis=1, keepdims=True) + eps)
        projected = projected + jnp.dot(
            (attended * norm * gain[...]).astype(BF16),
            weight[g * LANES : (g + 1) * LANES, :],
            preferred_element_type=F32,
        )
    out[...] = projected.astype(BF16)


def gate_body(attn, other, block, gate, up, both, sent, after):
    batch = attn.shape[0]
    rows = (block[:batch, :] + (attn[...] + other[...])).astype(BF16).astype(F32)
    after[...] = rows
    squares = jnp.sum(rows * rows, axis=1, keepdims=True)
    mixer_in = (rows * block[batch : batch + 1, :]).astype(BF16)
    width = gate.shape[1]
    for k, weight in enumerate((gate, up)):
        part = jnp.dot(mixer_in, weight[...], preferred_element_type=F32)
        both[:, k * width : (k + 1) * width] = part
        sent[:, k * width : (k + 1) * width] = part.astype(BF16)
    both[:, 2 * width :] = jnp.broadcast_to(squares, (batch, LANES))
    sent[:, 2 * width :] = high_and_low(squares, batch)


def high_and_low(squares, batch):
    high = squares.astype(BF16).astype(F32)
    low = lane_of((batch, LANES)) >= LANES // 2
    return jnp.where(low, squares - high, high).astype(BF16)


def gathered_sums(own, others):
    width = own.shape[1] - LANES
    sums = own[:, :width]
    squares = own[:, width : width + 1]
    for p in others:
        sums = sums + p[:, :width].astype(F32)
        tail = p[:, width:].astype(F32)
        squares = squares + (tail[:, :1] + tail[:, LANES // 2 : LANES // 2 + 1])
    return sums, squares


def middle_body(own, a, b, c, both, sent):
    sums, squares = gathered_sums(own, (a, b, c))
    batch, width = sums.shape
    both[:, :width] = sums
    sent[:, :width] = sums.astype(BF16)
    both[:, width:] = jnp.broadcast_to(squares, (batch, LANES))
    sent[:, width:] = high_and_low(squares, batch)


def down_body(own, a, b, c, weight, out):
    sums, squares = gathered_sums(own, (a, b, c))
    width = sums.shape[1] // 2
    inv = lax.rsqrt(squares / D + eps)
    gate, up = sums[:, :width] * inv, sums[:, width:] * inv
    hidden = (gate / (1.0 + jnp.exp(-gate)) * up).astype(BF16)
    out[...] = jnp.dot(hidden, weight[...], preferred_element_type=F32).astype(BF16)


def per_device(
    hidden_in,
    attn_gain,
    query_weight,
    key_cache,
    value_cache,
    lambdas,
    head_gain,
    out_weight,
    mixer_gain,
    gate_weight,
    up_weight,
    down_weight,
):
    batch, cols = hidden_in.shape
    width_q = query_weight.shape[1]
    heads = width_q // LANES
    wide = query_weight.shape[0]
    positions = key_cache.shape[1]
    shape = jax.ShapeDtypeStruct
    core = lax.axis_index(TP[1])
    chip = lax.axis_index(TP[0]).astype(jnp.int32)

    own = pl.pallas_call(
        pack_body,
        out_shape=shape((batch + 8, LANES), F32),
        in_specs=[pl.BlockSpec(memory_space=pltpu.HBM)] * 2,
        out_specs=pl.BlockSpec(memory_space=pltpu.VMEM),
        scratch_shapes=[
            pltpu.VMEM((batch, cols), BF16),
            pltpu.VMEM((1, cols), F32),
            pltpu.SemaphoreType.DMA((2,)),
        ],
        compiler_params=pltpu.CompilerParams(vmem_limit_bytes=4 * 2**20),
        cost_estimate=pl.CostEstimate(flops=COST, bytes_accessed=COST, transcendentals=0),
    )(
        pltpu.with_memory_space_constraint(hidden_in, pltpu.HBM),
        pltpu.with_memory_space_constraint(mixer_gain[None], pltpu.HBM),
    )
    mine = lane_of(own.shape) // cols % 2 == core
    pair = jnp.where(mine, own, partner(own))
    packed, block = kernel_call(
        query_body,
        [shape((heads * batch + 8, LANES), F32), shape((own.shape[0], wide), F32)],
        [pltpu.VMEM((4, *own.shape), F32)],
        smem=1,
        n_in=7,
        cost=COST,
    )(chip[None], pair, *peers(pair, "tp_0", "rows"), attn_gain[None], query_weight)
    packed = added(partner(packed), peers(packed, "kv_1", "query"))
    rows = batch * 2 * heads
    states = [shape((rows + 8, LANES), F32), shape((rows + 16, LANES), BF16)]
    state, sent = kernel_call(
        attend_body,
        states,
        [
            pltpu.VMEM((heads * batch, LANES), F32),
            pltpu.VMEM((2 * heads * batch, positions), F32),
            pltpu.VMEM((batch, 2 * heads, positions), BF16),
        ],
        n_in=6,
    )(
        partner(packed),
        *peers(packed, "kv_0", "query"),
        key_cache.reshape(batch, positions, LANES),
        value_cache.reshape(batch, positions, LANES),
    )
    state, sent = kernel_call(merge_body, states, n_in=4)(
        partner(state), *peers(sent, "kv_1", "heads")
    )
    projected = kernel_call(
        project_body,
        [shape((batch, wide), BF16)],
        [pltpu.VMEM((2 * heads * batch, LANES), F32)],
        n_in=7,
    )(lambdas[None], partner(state), *peers(sent, "kv_0", "heads"), head_gain[None], out_weight)[0]
    attn = added(
        projected.astype(F32), [p.astype(F32) for p in peers(projected, "tp_0", "attn")]
    )
    width = gate_weight.shape[1]
    both_shape = (batch, 2 * width + LANES)
    both, sent, after = kernel_call(
        gate_body,
        [shape(both_shape, F32), shape(both_shape, BF16), shape((batch, wide), F32)],
        n_in=5,
    )(attn, partner(attn), block, gate_weight, up_weight)
    both, sent = kernel_call(
        middle_body, [shape(both_shape, F32), shape(both_shape, BF16)], n_in=4
    )(both, *peers(sent, "kv_1", "gates"))
    down = kernel_call(down_body, [shape((batch, wide), BF16)], n_in=5)(
        both, *peers(sent, "kv_0", "gates"), down_weight
    )[0]
    mix = added(down.astype(F32), [p.astype(F32) for p in peers(down, "tp_0", "mix")])
    mixed = after + (mix + partner(mix))
    return lax.dynamic_slice_in_dim(mixed, (chip * 2 + core) * cols, cols, 1).astype(BF16)


def solution(mesh):
    split = Mesh(mesh.devices.reshape(4, 4, 4, 2), ("kv_0", "kv_1", "tp_0", "tp_1"))
    placed = (
        P(None, KV_TP),
        P(KV),
        P(KV, TP),
        P(None, KV, TP, None),
        P(None, KV, TP, None),
        P(TP),
        P(),
        P(TP, KV),
        P(KV_TP),
        P(KV, TP),
        P(KV, TP),
        P(TP, KV),
    )
    return jax.shard_map(
        per_device, mesh=split, in_specs=placed, out_specs=P(None, KV_TP), check_vma=False
    )
```
